128 devices in a mesh: sp: 16 (over z, y), tp: 8 (over x, core).
Axes of the slice: x: 4, y: 4, z: 4, core: 2. Of those that a mesh axis runs over, the one named last changes fastest.
Arguments:
- hidden: bfloat16 [6144, 4096], P('sp', 'tp'), may hold values from -6 to 6
- doc_ids: int32 [6144], P('sp'), may hold values from 0 to 7, never falling along the last dimension, each value on 1 to 1536 neighbouring positions
- norm_gain: float32 [3, 4096], replicated, may hold values from 0.1 to 1.9
- w_value: bfloat16 [3, 4096, 2048], P(None, 'sp', 'tp'), may hold values from -0.09375 to 0.09375
- w_gate: bfloat16 [3, 4096, 2048], P(None, 'sp', 'tp'), may hold values from -0.09375 to 0.09375
- conv_taps: float32 [3, 31, 2048], P(None, None, 'tp'), may hold values from -1 to 1
- conv_bias: float32 [3, 2048], P(None, 'tp'), may hold values from -3 to 3
- chan_gain: float32 [3, 2048], P(None, 'tp'), may hold values from 0.1 to 1.9
- chan_bias: float32 [3, 2048], P(None, 'tp'), may hold values from -3 to 3
- w_out: bfloat16 [3, 2048, 4096], P(None, 'sp', 'tp'), may hold values from -0.125 to 0.125
Outputs:
- result: bfloat16 [6144, 4096], P('sp', 'tp')
The draws below stay inside these ranges and needn't reach their ends.
Inputs may be any that keep to these rules, and one draw needn't show every extreme that they name: `doc_ids`: document numbers never fall along the sequence; each document has 1 to 1536 positions and one has exactly that many.
All inputs are finite; a program needn't handle non-finite values.
Results may differ from the reference program's by a relative error of at most 0.013.
Values may be sent and summed in bfloat16 or wider, within the bound.
No kernel may reach another device: no remote copies, remote signals or barrier semaphores. Data moves between devices by JAX's collectives and lax.ppermute only.
A program may use at most 128 MiB of HBM per device.

```python
import math
import jax
import jax.numpy as jnp
import numpy as np
from jax import lax

D = 4096
C = 2048
CONV_WIDTH = 31
LAYERS = 3
TOK_DEV = 384
TOKENS = 6144
DOCS = 8


def levels(own_key, extent, shards, low, largest):
    level = 1.0
    for position, shards_of in shards:
        steps = jax.random.uniform(jax.random.fold_in(jax.random.fold_in(own_key, 6), position), (shards_of,), jnp.float32, low / len(shards), largest / len(shards))
        level = level * jnp.repeat(jnp.exp(steps), extent[position] // shards_of).reshape((-1,) + (1,) * (len(extent) - 1 - position))
    return level


def profile(count, total, most, lean):
    loads = [(1 << 20) // math.isqrt(grade ** lean) + 1 for grade in range(2, count + 1)]
    rest, counts = total - most - (count - 1), [1] * (count - 1)
    while rest > 0:
        free = [i for i in range(count - 1) if counts[i] < most]
        mass, left = sum([loads[i] for i in free]), rest
        for i in free:
            more = min(most - counts[i], max(1, left * loads[i] // mass), rest)
            counts[i] = counts[i] + more
            rest = rest - more
    return np.array([most] + counts)


def uneven_parts(stream_key, amount, total, limit, lean):
    if amount == 2:
        one = jax.random.randint(stream_key, (), max(1, total - limit), min(limit, total - 1) + 1)
        return jnp.stack([one, total - one])
    lengths = jnp.asarray(profile(amount, total, limit, lean), jnp.int32)
    twos = (amount - 1) // 2
    donor, taker = lengths[1:1 + 2 * twos:2], lengths[2:2 + 2 * twos:2]
    margin = jnp.minimum(donor - 1, limit - taker)
    passed = jax.random.randint(jax.random.fold_in(stream_key, 1), (twos,), 0, 1 << 20) % (margin + 1)
    lengths = lengths.at[1:1 + 2 * twos:2].set(donor - passed).at[2:2 + 2 * twos:2].set(taker + passed)
    return lengths[jax.random.permutation(jax.random.fold_in(stream_key, 2), amount)]


def scatter_about(own_key, shape, scale, reach, pieces=(), dtype=jnp.bfloat16):
    loudness = levels(own_key, shape, pieces, -0.22, 0.18) if pieces else 1.0
    drawn = jax.random.normal(own_key, shape, jnp.float32) * scale * loudness
    return jnp.minimum(jnp.maximum(drawn, -reach), reach).astype(dtype)


def setup_inputs(seed: int = 0) -> dict:
    arg_keys = jax.random.split(jax.random.key(seed), 11)
    hidden = scatter_about(arg_keys[0], (TOKENS, D), 1.0, 6.0, ((0, 16), (1, 8)))
    doc_ids = jnp.searchsorted(jnp.cumsum(uneven_parts(arg_keys[1], DOCS, TOKENS, 4 * TOK_DEV, 0)), jnp.arange(TOKENS), side="right").astype(jnp.int32)
    norm_gain = jnp.clip(1.0 + 0.18 * jax.random.normal(arg_keys[2], (LAYERS, D), jnp.float32), 0.1, 1.9)
    w_value = scatter_about(arg_keys[3], (LAYERS, D, C), D ** -0.5, 0.09375, ((1, 16), (2, 8)))
    w_gate = scatter_about(arg_keys[4], (LAYERS, D, C), D ** -0.5, 0.09375, ((1, 16), (2, 8)))
    conv_taps = scatter_about(arg_keys[5], (LAYERS, CONV_WIDTH, C), CONV_WIDTH ** -0.5, 1.0, ((2, 8),), jnp.float32)
    conv_bias = scatter_about(arg_keys[6], (LAYERS, C), 0.5, 3.0, ((1, 8),), jnp.float32)
    chan_gain = jnp.clip(1.0 + 0.18 * jax.random.normal(arg_keys[7], (LAYERS, C), jnp.float32), 0.1, 1.9)
    chan_bias = scatter_about(arg_keys[8], (LAYERS, C), 0.5, 3.0, ((1, 8),), jnp.float32)
    w_out = scatter_about(arg_keys[9], (LAYERS, C, D), C ** -0.5, 0.125, ((1, 16), (2, 8)))
    return {"hidden": hidden, "doc_ids": doc_ids, "norm_gain": norm_gain, "w_value": w_value, "w_gate": w_gate, "conv_taps": conv_taps, "conv_bias": conv_bias, "chan_gain": chan_gain, "chan_bias": chan_bias, "w_out": w_out}


def one_layer(hidden, doc_ids, norm_gain, w_value, w_gate, conv_taps, conv_bias, chan_gain, chan_bias, w_out):
    width = conv_taps.shape[0]
    length = hidden.shape[0]
    xfloat = hidden.astype(jnp.float32)
    scale = lax.rsqrt(lax.optimization_barrier(jnp.mean(xfloat * xfloat, axis=-1, keepdims=True)) + 1e-06)
    normed = (xfloat * scale * norm_gain).astype(jnp.bfloat16)
    value = jnp.dot(normed, w_value, preferred_element_type=jnp.float32)
    gate = jnp.dot(normed, w_gate, preferred_element_type=jnp.float32)
    glu = (value * jax.nn.sigmoid(gate)).astype(jnp.bfloat16)
    padded = jnp.concatenate([jnp.zeros((width - 1, glu.shape[1]), jnp.float32), glu.astype(jnp.float32)], axis=0)
    seg_pad = jnp.concatenate([jnp.full((width - 1,), -1, jnp.int32), doc_ids.astype(jnp.int32)], axis=0)
    conv = jnp.zeros(glu.shape, jnp.float32) + conv_bias
    for index in range(width):
        source = padded[index:index + length]
        keep = (seg_pad[index:index + length] == doc_ids)[:, None]
        conv = conv + jnp.where(keep, source * conv_taps[index], 0.0)
    mean_val = lax.optimization_barrier(jnp.mean(conv, axis=-1, keepdims=True))
    var_val = lax.optimization_barrier(jnp.mean(conv * conv, axis=-1, keepdims=True)) - mean_val * mean_val
    mixed = jax.nn.silu((conv - mean_val) * lax.rsqrt(var_val + 1e-05) * chan_gain + chan_bias).astype(jnp.bfloat16)
    return (xfloat + jnp.dot(mixed, w_out, preferred_element_type=jnp.float32)).astype(jnp.bfloat16)

def reference(hidden, doc_ids, norm_gain, w_value, w_gate, conv_taps, conv_bias, chan_gain, chan_bias, w_out):
    state = hidden
    for layer in range(LAYERS):
        state = one_layer(state, doc_ids, norm_gain[layer], w_value[layer], w_gate[layer], conv_taps[layer], conv_bias[layer], chan_gain[layer], chan_bias[layer], w_out[layer])
    return state
```

```python
import functools

import jax
import jax.numpy as jnp
from jax import lax
from jax.experimental import pallas as pl
from jax.experimental.pallas import tpu as pltpu
from jax.sharding import Mesh, PartitionSpec as P

LAYERS = 3
T = 192
HALO = 32
TAPS = 31
F32 = jnp.float32
BF16 = jnp.bfloat16


def shift(a, axis, by):
    return lax.ppermute(a, axis, [(i, (i + by) % 4) for i in range(4)])


def swap(a):
    return lax.ppermute(a, "c", [(0, 1), (1, 0)])


def around(a, axis):
    one, three, two = shift(a, axis, 1), shift(a, axis, 3), shift(a, axis, 2)
    return [a, one, two, three]


def row_block(ix, e, d):
    return ((ix[2] - e) & 3) * 4 + ((ix[1] - d) & 3)


def own_block(ix, d, half, q):
    core = ix[3] if half == 0 else 1 - ix[3]
    return ((ix[0] - d) & 3) * 4 + core * 2 + q


def glu_kernel(ix, *refs):
    xp, gain, (out, xs, accv, accg) = refs[:4], refs[4], refs[-4:]
    w = refs[5:-4]
    v_own, v_oth, g_own, g_oth = w[:4], w[4:8], w[8:12], w[12:16]
    i = pl.program_id(0)

    @pl.when(i == 0)
    def _():
        ss = jnp.zeros((T, 1), F32)
        for d in range(4):
            for h in range(2):
                xf = xp[d][h * T : (h + 1) * T, :].astype(F32)
                ss = ss + jnp.sum(xf * xf, axis=1, keepdims=True)
        scale = lax.rsqrt(ss / 4096.0 + 1e-6)
        for d in range(4):
            for h in range(2):
                for q in range(2):
                    b = own_block(ix, d, h, q)
                    xf = xp[d][h * T : (h + 1) * T, q * 256 : (q + 1) * 256].astype(F32)
                    xs[b] = (xf * scale * gain[b]).astype(BF16)
        accv[...] = jnp.zeros_like(accv)
        accg[...] = jnp.zeros_like(accg)

    def both(own, oth):
        return jnp.concatenate(
            [
                jnp.concatenate([r[0] for r in own], axis=0),
                jnp.concatenate([r[0] for r in oth], axis=0),
            ],
            axis=1,
        )

    xv = jnp.concatenate([xs[row_block(ix, e, i)] for e in range(4)], axis=1)
    accv[...] += jnp.dot(xv, both(v_own, v_oth), preferred_element_type=F32)
    xg = jnp.concatenate([xs[row_block(ix, i, d)] for d in range(4)], axis=1)
    accg[...] += jnp.dot(xg, both(g_own, g_oth), preferred_element_type=F32)

    @pl.when(i == 3)
    def _():
        glu = (accv[...] * jax.nn.sigmoid(accg[...])).astype(BF16)
        out[...] = glu


def glu_call(ix, xp, gain, weights):
    whole = lambda shape: pl.BlockSpec(shape, lambda i, s: (0,) * len(shape))
    piece = pl.BlockSpec((1, 256, 256), lambda i, s: (i, 0, 0))
    return pl.pallas_call(
        glu_kernel,
        grid_spec=pltpu.PrefetchScalarGridSpec(
            num_scalar_prefetch=1,
            grid=(4,),
            in_specs=[whole((2 * T, 512))] * 4 + [whole((16, 1, 256))] + [piece] * 16,
            out_specs=whole((T, 512)),
            scratch_shapes=[
                pltpu.VMEM((16, T, 256), BF16),
                pltpu.VMEM((T, 512), F32),
                pltpu.VMEM((T, 512), F32),
            ],
        ),
        out_shape=jax.ShapeDtypeStruct((T, 512), BF16),
        cost_estimate=pl.CostEstimate(
            flops=2 * T * 4096 * 1024, bytes_accessed=10 * 2**20, transcendentals=0
        ),
        name="glu",
    )(ix, *xp, gain, *weights)


def conv_kernel(halo, glu, lim, taps, bias, out, ext):
    for j in range(4):
        ext[j, HALO:, :] = glu[:, j * 128 : (j + 1) * 128].astype(F32)
        k = (j + 2) % 4
        ext[j, :HALO, :] = halo[:, k * 128 : (k + 1) * 128].astype(F32)
    lane = lax.broadcasted_iota(jnp.int32, (32, 128), 1)
    row = lax.broadcasted_iota(jnp.int32, (32, 128), 0)
    means = [jnp.zeros((1, 128), F32), jnp.zeros((1, 128), F32)]
    for r in range(0, T, 32):
        reach = lim[r : r + 32, :]
        acc = [jnp.broadcast_to(bias[:, j * 128 : (j + 1) * 128], (32, 128)) for j in range(4)]
        for i in range(TAPS):
            keep = reach >= (TAPS - 1 - i)
            at = r + HALO - (TAPS - 1) + i
            for j in range(4):
                term = ext[j, at : at + 32, :] * taps[i : i + 1, j * 128 : (j + 1) * 128]
                acc[j] = acc[j] + jnp.where(keep, term, 0.0)
        mean = jnp.sum(acc[0] + acc[1] + acc[2] + acc[3], axis=1, keepdims=True) / 512.0
        mean = mean.astype(BF16).astype(F32)
        for j in range(4):
            out[r : r + 32, j * 128 : (j + 1) * 128] = (acc[j] - mean).astype(BF16)
        spot = jnp.where(lane == row + r % 128, mean, 0.0)
        means[r // 128] = means[r // 128] + jnp.sum(spot, axis=0, keepdims=True)
    pick = lax.broadcasted_iota(jnp.int32, (16, 128), 0)
    tail = jnp.where(pick == 0, means[0], jnp.where(pick == 1, means[1], 0.0))
    out[T:, :128] = tail.astype(BF16)
    out[T:, 128:] = jnp.zeros((16, 384), BF16)


def conv_call(halo, glu, lim, taps, bias):
    return pl.pallas_call(
        conv_kernel,
        out_shape=jax.ShapeDtypeStruct((T + 16, 512), BF16),
        scratch_shapes=[pltpu.VMEM((4, HALO + T, 128), F32)],
        cost_estimate=pl.CostEstimate(flops=10**9, bytes_accessed=2**20, transcendentals=0),
        name="conv",
    )(halo, glu, lim, taps, bias)


def mix_kernel(ix, *refs):
    cp, gb, state, (out, cv, ms, acca, accb) = refs[:4], refs[4:8], refs[8], refs[-5:]
    w = refs[9:-5]
    a_own, a_oth, b_own, b_oth = w[:4], w[4:8], w[8:12], w[12:16]
    i = pl.program_id(0)

    @pl.when(i == 0)
    def _():
        lane = lax.broadcasted_iota(jnp.int32, (T, 128), 1)
        row = lax.broadcasted_iota(jnp.int32, (T, 128), 0)
        first = row < 128
        spot = lane == (row & 127)
        total = jnp.zeros((T, 1), F32)
        for d in range(4):
            tail = cp[d][T : T + 16, :128].astype(F32)
            mine = jnp.where(first, tail[0:1, :], tail[1:2, :])
            mean = jnp.sum(jnp.where(spot, mine, 0.0), axis=1, keepdims=True)
            conv = cp[d][:T, :].astype(F32) + mean
            cv[d] = conv
            total = total + jnp.sum(conv, axis=1, keepdims=True)
        mu = total / 2048.0
        square = jnp.zeros((T, 1), F32)
        for d in range(4):
            off = cv[d] - mu
            square = square + jnp.sum(off * off, axis=1, keepdims=True)
        inv = lax.rsqrt(square / 2048.0 + 1e-5)
        for d in range(4):
            for k in range(4):
                at = slice(k * 128, (k + 1) * 128)
                y = (cv[d, :, at] - mu) * inv * gb[d][0:1, at] + gb[d][1:2, at]
                ms[own_block(ix, d, k // 2, k % 2)] = (y * jax.nn.sigmoid(y)).astype(BF16)
        acca[...] = jnp.zeros_like(acca)
        accb[...] = jnp.zeros_like(accb)

    def both(own, oth):
        return jnp.concatenate(
            [
                jnp.concatenate([r[0] for r in own], axis=0),
                jnp.concatenate([r[0] for r in oth], axis=0),
            ],
            axis=1,
        )

    xa = jnp.concatenate([ms[row_block(ix, e, i)] for e in range(4)], axis=1)
    acca[...] += jnp.dot(xa, both(a_own, a_oth), preferred_element_type=F32)
    xb = jnp.concatenate([ms[row_block(ix, i, d)] for d in range(4)], axis=1)
    accb[...] += jnp.dot(xb, both(b_own, b_oth), preferred_element_type=F32)

    @pl.when(i == 3)
    def _():
        for h in range(2):
            at = slice(h * 256, (h + 1) * 256)
            rows = slice(h * T, (h + 1) * T)
            out[rows, :256] = (state[rows, :256].astype(F32) + acca[:, at]).astype(BF16)
            out[rows, 256:] = (state[rows, 256:].astype(F32) + accb[:, at]).astype(BF16)


def mix_call(ix, cp, gb, state, weights, at):
    whole = lambda shape: pl.BlockSpec(shape, lambda i, s: (0,) * len(shape))
    piece = pl.BlockSpec((1, 128, 256), lambda i, s: (i, at, 0))
    return pl.pallas_call(
        mix_kernel,
        grid_spec=pltpu.PrefetchScalarGridSpec(
            num_scalar_prefetch=1,
            grid=(4,),
            in_specs=[whole((T + 16, 512))] * 4
            + [whole((2, 512))] * 4
            + [whole((2 * T, 512))]
            + [piece] * 16,
            out_specs=whole((2 * T, 512)),
            scratch_shapes=[
                pltpu.VMEM((4, T, 512), F32),
                pltpu.VMEM((16, T, 128), BF16),
                pltpu.VMEM((T, 512), F32),
                pltpu.VMEM((T, 512), F32),
            ],
        ),
        out_shape=jax.ShapeDtypeStruct((2 * T, 512), BF16),
        cost_estimate=pl.CostEstimate(
            flops=2 * T * 2048 * 1024, bytes_accessed=6 * 2**20, transcendentals=0
        ),
        name="mix",
    )(ix, *cp, *gb, state, *weights)


def gathered(a, b):
    a = jnp.stack(around(a, "y"))
    b = jnp.stack(around(b, "z"))
    a = around(a, "z")
    b = around(b, "y")
    return (*a, *[swap(p) for p in a], *b, *[swap(p) for p in b])


def per_device(
    hidden, doc_ids, norm_gain, w_value, w_gate, conv_taps, conv_bias, chan_gain, chan_bias, w_out
):
    x, y, z, c = (lax.axis_index(n) for n in ("x", "y", "z", "c"))
    ix = jnp.stack([x, y, z, c]).astype(jnp.int32)

    own = lax.dynamic_slice_in_dim(hidden, c * T, T, 0)
    oth = swap(lax.dynamic_slice_in_dim(hidden, (1 - c) * T, T, 0))
    state = jnp.concatenate([own, oth], axis=0)

    glu_w = [gathered(w_value[0], w_gate[0])]
    mix_w = [gathered(w_out[0, :, :256], w_out[0, :, 256:])]
    for l in range(1, LAYERS):
        both = gathered(
            jnp.concatenate([w_value[l], w_out[l, :, :256]], axis=0),
            jnp.concatenate([w_gate[l], w_out[l, :, 256:]], axis=0),
        )
        glu_w.append(both)
        mix_w.append(both)

    small = jnp.concatenate(
        [conv_taps.reshape(LAYERS * TAPS, 256), conv_bias, chan_gain, chan_bias], axis=0
    )
    small = jnp.concatenate([small, swap(small)], axis=1)
    taps = small[: LAYERS * TAPS].reshape(LAYERS, TAPS, 512)
    bias = small[LAYERS * TAPS : LAYERS * TAPS + LAYERS]
    norm2 = around(small[LAYERS * TAPS + LAYERS :], "x")

    ring = [(i, i + 1) for i in range(15)]
    behind = lax.ppermute(doc_ids[-HALO:] + 1, ("z", "y"), ring) - 1
    docs = jnp.concatenate([behind, doc_ids])
    docs = lax.dynamic_slice_in_dim(docs, c * T, HALO + T, 0)
    mine = docs[HALO:]
    reach = sum((docs[HALO - o : HALO - o + T] == mine).astype(jnp.int32) for o in range(1, TAPS))
    lim = jnp.broadcast_to(reach[:, None], (T, 128))

    gains = norm_gain.reshape(LAYERS, 16, 1, 256)
    blocks = [(i, i + 1) for i in range(31)]
    for l in range(LAYERS):
        glu = glu_call(ix, around(state, "x"), gains[l], glu_w[l])
        halo = lax.ppermute(glu[-HALO:], ("z", "y", "c"), blocks)
        dev = conv_call(halo, glu, lim, taps[l], bias[l : l + 1])
        gb = [jnp.stack([p[l], p[LAYERS + l]]) for p in norm2]
        state = mix_call(ix, around(dev, "x"), gb, state, mix_w[l], 0 if l == 0 else 2)

    own, oth = state[:T], swap(state[T:])
    low = jnp.where(c == 0, own, oth)
    high = jnp.where(c == 0, oth, own)
    return jnp.concatenate([low, high], axis=0)


def solution(mesh):
    fine = Mesh(mesh.devices.reshape(4, 4, 4, 2), ("z", "y", "x", "c"))
    sp, tp = ("z", "y"), ("x", "c")
    placed = (
        P(sp, tp),
        P(sp),
        P(),
        P(None, sp, tp),
        P(None, sp, tp),
        P(None, None, tp),
        P(None, tp),
        P(None, tp),
        P(None, tp),
        P(None, sp, tp),
    )
    return jax.shard_map(
        per_device, mesh=fine, in_specs=placed, out_specs=P(sp, tp), check_vma=False
    )
```

```python
import jax
import jax.numpy as jnp
from jax import lax
from jax.experimental import pallas as pl
from jax.experimental.pallas import tpu as pltpu
from jax.sharding import Mesh, PartitionSpec as P

LAYERS = 3
T = 192
HALO = 32
TAPS = 31
F32 = jnp.float32
BF16 = jnp.bfloat16


def swap(a):
    return lax.ppermute(a, "c", [(0, 1), (1, 0)])


def to_all(a, axis):
    n = lax.axis_size(axis)
    return lax.all_to_all(jnp.broadcast_to(a[None], (n, *a.shape)), axis, 0, 0, tiled=True)


def dot(a, b):
    return jnp.dot(a, b, preferred_element_type=F32)


def in_order(w, c):
    return jnp.concatenate([w[2 * c], w[2 * c + 1], w[2 - 2 * c], w[3 - 2 * c]], axis=0)


def first_glu_kernel(ix, xp, gain, w, mine, other, ss, acc):
    i = pl.program_id(0)

    @pl.when(i == 0)
    def _():
        ss[...] = jnp.zeros_like(ss)
        acc[...] = jnp.zeros_like(acc)

    parts, square = [], ss[...]
    for j in range(2):
        xf = xp[j].astype(F32)
        square = square + jnp.sum(xf * xf, axis=1, keepdims=True)
        parts.append((xf * gain[0, :, j * 512 : (j + 1) * 512]).astype(BF16))
    ss[...] = square
    acc[...] += dot(jnp.concatenate(parts, axis=1), w[...].reshape(1024, 512))

    @pl.when(i == 3)
    def _():
        for h, out in ((ix[3], mine), (1 - ix[3], other)):
            rows = pl.ds(pl.multiple_of(h * T, T), T)
            scale = lax.rsqrt(ss[rows] / 4096.0 + 1e-6)
            y = acc[rows, :] * scale
            out[...] = (y[:, :256] * jax.nn.sigmoid(y[:, 256:])).astype(BF16)


def first_glu_call(ix, xp, gain, w):
    return pl.pallas_call(
        first_glu_kernel,
        grid_spec=pltpu.PrefetchScalarGridSpec(
            num_scalar_prefetch=1,
            grid=(4,),
            in_specs=[
                pl.BlockSpec((2, 2 * T, 512), lambda i, s: (i, 0, 0)),
                pl.BlockSpec((1, 1, 1024), lambda i, s: (i, 0, 0)),
                pl.BlockSpec((4, 256, 512), lambda i, s: (i, 0, 0)),
            ],
            out_specs=[pl.BlockSpec((T, 256), lambda i, s: (0, 0))] * 2,
            scratch_shapes=[pltpu.VMEM((2 * T, 1), F32), pltpu.VMEM((2 * T, 512), F32)],
        ),
        out_shape=[jax.ShapeDtypeStruct((T, 256), BF16)] * 2,
        cost_estimate=pl.CostEstimate(
            flops=2 * T * 4096 * 1024, bytes_accessed=8 * 2**20, transcendentals=0
        ),
        name="glu0",
    )(ix, xp, gain.reshape(4, 1, 1024), w)


def glu_kernel(ix, xp, gain, w_own, w_oth, own, oth, edge, ss, acc_own, acc_oth):
    i, c = pl.program_id(0), ix[3]

    @pl.when(i == 0)
    def _():
        ss[...] = jnp.zeros_like(ss)
        acc_own[...] = jnp.zeros_like(acc_own)
        acc_oth[...] = jnp.zeros_like(acc_oth)

    parts, square = [], ss[...]
    for h, core in ((0, c), (1, 1 - c)):
        xf = xp[0, h * T : (h + 1) * T, :].astype(F32)
        square = square + jnp.sum(xf * xf, axis=1, keepdims=True)
        parts.append((xf * gain[0, core]).astype(BF16))
    ss[...] = square
    x = jnp.concatenate(parts, axis=1)
    acc_own[...] += dot(x, in_order(w_own, c))
    acc_oth[...] += dot(x, in_order(w_oth, c))

    @pl.when(i == 3)
    def _():
        scale = lax.rsqrt(ss[...] / 4096.0 + 1e-6)
        for h, (acc, out) in enumerate(((acc_own, own), (acc_oth, oth))):
            y = acc[...] * scale
            glu = (y[:, :256] * jax.nn.sigmoid(y[:, 256:])).astype(BF16)
            out[...] = glu
            edge[h * HALO : (h + 1) * HALO, :] = glu[T - HALO :, :]


def glu_call(ix, xp, gain, w_own, w_oth, at):
    piece = pl.BlockSpec((4, 256, 512), lambda i, s: (i, at, 0))
    return pl.pallas_call(
        glu_kernel,
        grid_spec=pltpu.PrefetchScalarGridSpec(
            num_scalar_prefetch=1,
            grid=(4,),
            in_specs=[
                pl.BlockSpec((1, 2 * T, 512), lambda i, s: (i, 0, 0)),
                pl.BlockSpec((1, 2, 1, 512), lambda i, s: (i, 0, 0, 0)),
                piece,
                piece,
            ],
            out_specs=[
                pl.BlockSpec((T, 256), lambda i, s: (0, 0)),
                pl.BlockSpec((T, 256), lambda i, s: (0, 0)),
                pl.BlockSpec((2 * HALO, 256), lambda i, s: (0, 0)),
            ],
            scratch_shapes=[
                pltpu.VMEM((T, 1), F32),
                pltpu.VMEM((T, 512), F32),
                pltpu.VMEM((T, 512), F32),
            ],
        ),
        out_shape=[
            jax.ShapeDtypeStruct((T, 256), BF16),
            jax.ShapeDtypeStruct((T, 256), BF16),
            jax.ShapeDtypeStruct((2 * HALO, 256), BF16),
        ],
        cost_estimate=pl.CostEstimate(
            flops=2 * T * 4096 * 1024, bytes_accessed=10 * 2**20, transcendentals=0
        ),
        name="glu",
    )(ix, xp, gain.reshape(4, 2, 1, 512), w_own, w_oth)


def conv_kernel(edge, own, oth, lim, taps, bias, out, ext):
    for j in range(4):
        cols = slice(j % 2 * 128, j % 2 * 128 + 128)
        ext[j, HALO:, :] = (own, oth)[j // 2][:, cols].astype(F32)
        rows = slice((1 - j // 2) * HALO, (2 - j // 2) * HALO)
        ext[j, :HALO, :] = edge[rows, cols].astype(F32)
    lane = lax.broadcasted_iota(jnp.int32, (32, 128), 1)
    row = lax.broadcasted_iota(jnp.int32, (32, 128), 0)
    means = [jnp.zeros((1, 128), F32), jnp.zeros((1, 128), F32)]
    for r in range(0, T, 32):
        reach = lim[r : r + 32, :]
        acc = [jnp.broadcast_to(bias[:, j * 128 : (j + 1) * 128], (32, 128)) for j in range(4)]
        for i in range(TAPS):
            keep = reach >= (TAPS - 1 - i)
            at = r + HALO - (TAPS - 1) + i
            for j in range(4):
                term = ext[j, at : at + 32, :] * taps[i : i + 1, j * 128 : (j + 1) * 128]
                acc[j] = acc[j] + jnp.where(keep, term, 0.0)
        mean = jnp.sum(acc[0] + acc[1] + acc[2] + acc[3], axis=1, keepdims=True) / 512.0
        mean = mean.astype(BF16).astype(F32)
        for j in range(4):
            dev = (acc[j] - mean).astype(BF16)
            for k in range(4):
                out[k, r : r + 32, j * 128 : (j + 1) * 128] = dev
        spot = jnp.where(lane == row + r % 128, mean, 0.0)
        means[r // 128] = means[r // 128] + jnp.sum(spot, axis=0, keepdims=True)
    pick = lax.broadcasted_iota(jnp.int32, (16, 128), 0)
    tail = jnp.where(pick == 0, means[0], jnp.where(pick == 1, means[1], 0.0))
    for k in range(4):
        out[k, T:, :128] = tail.astype(BF16)
        out[k, T:, 128:] = jnp.zeros((16, 384), BF16)


def conv_call(edge, own, oth, lim, taps, bias):
    return pl.pallas_call(
        conv_kernel,
        out_shape=jax.ShapeDtypeStruct((4, T + 16, 512), BF16),
        scratch_shapes=[pltpu.VMEM((4, HALO + T, 128), F32)],
        cost_estimate=pl.CostEstimate(flops=10**9, bytes_accessed=2**20, transcendentals=0),
        name="conv",
    )(edge, own, oth, lim, taps, bias)


def mix_kernel(ix, cp, gb, state, w_own, w_oth, out, mean, mu, inv, acc_own, acc_oth):
    i, c = pl.program_id(0), ix[3]

    @pl.when(i == 0)
    def _():
        lane = lax.broadcasted_iota(jnp.int32, (T, 128), 1)
        row = lax.broadcasted_iota(jnp.int32, (T, 128), 0)
        spot = lane == (row & 127)
        total = jnp.zeros((T, 1), F32)
        for d in range(4):
            tail = cp[d, T : T + 16, :128].astype(F32)
            mine = jnp.where(row < 128, tail[0:1, :], tail[1:2, :])
            m = jnp.sum(jnp.where(spot, mine, 0.0), axis=1, keepdims=True)
            mean[d] = m
            total = total + 512.0 * m + jnp.sum(cp[d, :T, :].astype(F32), axis=1, keepdims=True)
        center = total / 2048.0
        mu[...] = center
        square = jnp.zeros((T, 1), F32)
        for d in range(4):
            off = cp[d, :T, :].astype(F32) + (mean[d] - center)
            square = square + jnp.sum(off * off, axis=1, keepdims=True)
        inv[...] = lax.rsqrt(square / 2048.0 + 1e-5)
        acc_own[...] = jnp.zeros_like(acc_own)
        acc_oth[...] = jnp.zeros_like(acc_oth)

    off = cp[i, :T, :].astype(F32) + (mean[i] - mu[...])
    y = off * inv[...] * gb[i, 0:1, :] + gb[i, 1:2, :]
    mixed = (y * jax.nn.sigmoid(y)).astype(BF16)
    acc_own[...] += dot(mixed, in_order(w_own, c))
    acc_oth[...] += dot(mixed, in_order(w_oth, c))

    @pl.when(i == 3)
    def _():
        for h, acc in enumerate((acc_own, acc_oth)):
            rows = slice(h * T, (h + 1) * T)
            out[rows, :] = (state[rows, :].astype(F32) + acc[...]).astype(BF16)


def mix_call(ix, cp, gb, state, w_own, w_oth, at):
    whole = lambda *shape: pl.BlockSpec(shape, lambda i, s: (0,) * len(shape))
    piece = pl.BlockSpec((4, 128, 512), lambda i, s: (i, at, 0))
    return pl.pallas_call(
        mix_kernel,
        grid_spec=pltpu.PrefetchScalarGridSpec(
            num_scalar_prefetch=1,
            grid=(4,),
            in_specs=[whole(4, T + 16, 512), whole(4, 2, 512), whole(2 * T, 512), piece, piece],
            out_specs=whole(2 * T, 512),
            scratch_shapes=[
                pltpu.VMEM((4, T, 1), F32),
                pltpu.VMEM((T, 1), F32),
                pltpu.VMEM((T, 1), F32),
                pltpu.VMEM((T, 512), F32),
                pltpu.VMEM((T, 512), F32),
            ],
        ),
        out_shape=jax.ShapeDtypeStruct((2 * T, 512), BF16),
        cost_estimate=pl.CostEstimate(
            flops=2 * T * 2048 * 1024, bytes_accessed=6 * 2**20, transcendentals=0
        ),
        name="mix",
    )(ix, cp, gb, state, w_own, w_oth)


def per_device(
    hidden, doc_ids, norm_gain, w_value, w_gate, conv_taps, conv_bias, chan_gain, chan_bias, w_out
):
    x, y, z, c = (lax.axis_index(n) for n in ("x", "y", "z", "c"))
    ix = jnp.stack([x, y, z, c]).astype(jnp.int32)

    pair = jnp.concatenate([w_value, w_gate], axis=2)
    early = jnp.concatenate([pair[0], pair[1], w_out[0]], axis=0)
    late = jnp.concatenate([pair[2], w_out[1], w_out[2]], axis=0)
    early = lax.all_gather(early, ("z", "y"), axis=0)
    late = lax.all_gather(late, ("z", "y"), axis=0)
    early2, late2 = swap(early), swap(late)

    first = to_all(hidden, ("x", "c"))

    own = lax.dynamic_slice_in_dim(hidden, c * T, T, 0)
    oth = swap(lax.dynamic_slice_in_dim(hidden, (1 - c) * T, T, 0))
    state = jnp.concatenate([own, oth], axis=0)

    small = jnp.concatenate(
        [conv_taps.reshape(LAYERS * TAPS, 256), conv_bias, chan_gain, chan_bias], axis=0
    )
    small = jnp.concatenate([small, swap(small)], axis=1)
    taps = small[: LAYERS * TAPS].reshape(LAYERS, TAPS, 512)
    bias = small[LAYERS * TAPS : LAYERS * TAPS + LAYERS]
    norm2 = to_all(small[LAYERS * TAPS + LAYERS :], "x").reshape(4, 2, LAYERS, 512)

    ring = [(i, i + 1) for i in range(15)]
    behind = lax.ppermute(doc_ids[-HALO:] + 1, ("z", "y"), ring) - 1
    docs = jnp.concatenate([behind, doc_ids])
    docs = lax.dynamic_slice_in_dim(docs, c * T, HALO + T, 0)
    here = docs[HALO:]
    reach = sum((docs[HALO - o : HALO - o + T] == here).astype(jnp.int32) for o in range(1, TAPS))
    lim = jnp.broadcast_to(reach[:, None], (T, 128))

    blocks = [(i, i + 1) for i in range(31)]
    glu_at = (None, (early, early2, 1), (late, late2, 0))
    mix_at = ((early, early2, 4), (late, late2, 2), (late, late2, 3))
    for l in range(LAYERS):
        if l == 0:
            own, other = first_glu_call(ix, first, norm_gain[l], early)
            oth = swap(other)
            edge = jnp.concatenate([own[-HALO:], oth[-HALO:]], axis=0)
        else:
            own, oth, edge = glu_call(ix, to_all(state, "x"), norm_gain[l], *glu_at[l])
        edge = lax.ppermute(edge, ("z", "y", "c"), blocks)
        dev = conv_call(edge, own, oth, lim, taps[l], bias[l : l + 1])
        dev = lax.all_to_all(dev, "x", 0, 0, tiled=True)
        state = mix_call(ix, dev, norm2[:, :, l], state, *mix_at[l])

    own, oth = state[:T], swap(state[T:])
    low = jnp.where(c == 0, own, oth)
    high = jnp.where(c == 0, oth, own)
    return jnp.concatenate([low, high], axis=0)


def solution(mesh):
    fine = Mesh(mesh.devices.reshape(4, 4, 4, 2), ("z", "y", "x", "c"))
    sp, tp = ("z", "y"), ("x", "c")
    placed = (
        P(sp, tp),
        P(sp),
        P(),
        P(None, sp, tp),
        P(None, sp, tp),
        P(None, None, tp),
        P(None, tp),
        P(None, tp),
        P(None, tp),
        P(None, sp, tp),
    )
    return jax.shard_map(
        per_device, mesh=fine, in_specs=placed, out_specs=P(sp, tp), check_vma=False
    )
```

```python
import functools

import jax
import jax.numpy as jnp
from jax import lax
from jax.experimental import pallas as pl
from jax.experimental.pallas import tpu as pltpu
from jax.sharding import Mesh, PartitionSpec as P

LAYERS = 3
T = 192
HALO = 32
TAPS = 31
F32 = jnp.float32
BF16 = jnp.bfloat16


def swap(a):
    return lax.ppermute(a, "c", [(0, 1), (1, 0)])


def shift(a, by):
    return lax.ppermute(a, "x", [(i, (i + by) % 4) for i in range(4)])


def ring(a, b):
    left_a, right_b = shift(a, 1), shift(b, 3)
    left_b, right_a = shift(b, 1), shift(a, 3)
    return a, b, left_a, left_b, shift(left_a, 1), shift(right_b, 3), right_a, right_b


def to_all(a, axis):
    n = lax.axis_size(axis)
    return lax.all_to_all(jnp.broadcast_to(a[None], (n, *a.shape)), axis, 0, 0, tiled=True)


def dot(a, b):
    return jnp.dot(a, b, preferred_element_type=F32)


def in_order(w, c):
    return jnp.concatenate([w[2 * c], w[2 * c + 1], w[2 - 2 * c], w[3 - 2 * c]], axis=0)


def first_glu_kernel(ix, xp, gain, w, mine, other, ss, acc):
    i = pl.program_id(0)

    @pl.when(i == 0)
    def _():
        ss[...] = jnp.zeros_like(ss)
        acc[...] = jnp.zeros_like(acc)

    parts, square = [], ss[...]
    for j in range(2):
        xf = xp[j].astype(F32)
        square = square + jnp.sum(xf * xf, axis=1, keepdims=True)
        parts.append((xf * gain[0, :, j * 512 : (j + 1) * 512]).astype(BF16))
    ss[...] = square
    acc[...] += dot(jnp.concatenate(parts, axis=1), w[...].reshape(1024, 512))

    @pl.when(i == 3)
    def _():
        for h, out in ((ix[3], mine), (1 - ix[3], other)):
            rows = pl.ds(pl.multiple_of(h * T, T), T)
            scale = lax.rsqrt(ss[rows] / 4096.0 + 1e-6)
            y = acc[rows, :] * scale
            out[...] = (y[:, :256] * jax.nn.sigmoid(y[:, 256:])).astype(BF16)


def first_glu_call(ix, xp, gain, w):
    return pl.pallas_call(
        first_glu_kernel,
        grid_spec=pltpu.PrefetchScalarGridSpec(
            num_scalar_prefetch=1,
            grid=(4,),
            in_specs=[
                pl.BlockSpec((2, 2 * T, 512), lambda i, s: (i, 0, 0)),
                pl.BlockSpec((1, 1, 1024), lambda i, s: (i, 0, 0)),
                pl.BlockSpec((4, 256, 512), lambda i, s: (i, 0, 0)),
            ],
            out_specs=[pl.BlockSpec((T, 256), lambda i, s: (0, 0))] * 2,
            scratch_shapes=[pltpu.VMEM((2 * T, 1), F32), pltpu.VMEM((2 * T, 512), F32)],
        ),
        out_shape=[jax.ShapeDtypeStruct((T, 256), BF16)] * 2,
        cost_estimate=pl.CostEstimate(
            flops=2 * T * 4096 * 1024, bytes_accessed=8 * 2**20, transcendentals=0
        ),
        name="glu0",
    )(ix, xp, gain.reshape(4, 1, 1024), w)


def fetch(src, row, rows, at, dst, sem):
    first = pl.multiple_of(row * 4, 4)
    copy = pltpu.make_async_copy(src.at[pl.ds(first, 4), pl.ds(at * rows, rows), :], dst, sem)
    copy.start()
    return copy


ARRIVAL = (0, 1, 3, 2)


def glu_kernel(at, ix, *refs):
    xp, gain, w_own, w_oth, own, oth, edge, buf, sem = refs[:8], *refs[8:]
    x, c = ix[0], ix[3]
    copies = [
        fetch(w, (x - d) & 3, 256, at, buf.at[h, n], sem.at[h, n])
        for n, d in enumerate(ARRIVAL)
        for h, w in enumerate((w_own, w_oth))
    ]
    square = jnp.zeros((T, 1), F32)
    acc = [jnp.zeros((T, 512), F32)] * 2
    for n, d in enumerate(ARRIVAL):
        parts = []
        for h, core in ((0, c), (1, 1 - c)):
            xf = xp[2 * d + h][...].astype(F32)
            square = square + jnp.sum(xf * xf, axis=1, keepdims=True)
            parts.append((xf * gain[((x - d) & 3) * 2 + core]).astype(BF16))
        rows = jnp.concatenate(parts, axis=1)
        for h in range(2):
            copies[2 * n + h].wait()
            acc[h] = acc[h] + dot(rows, in_order(buf.at[h, n], c))
    scale = lax.rsqrt(square / 4096.0 + 1e-6)
    for h, out in enumerate((own, oth)):
        y = acc[h] * scale
        glu = (y[:, :256] * jax.nn.sigmoid(y[:, 256:])).astype(BF16)
        out[...] = glu
        edge[h * HALO : (h + 1) * HALO, :] = glu[T - HALO :, :]


SMEM = pl.BlockSpec(memory_space=pltpu.SMEM)
VMEM = pl.BlockSpec(memory_space=pltpu.VMEM)
ANY = pl.BlockSpec(memory_space=pl.ANY)


def glu_call(ix, xp, gain, w_own, w_oth, at):
    return pl.pallas_call(
        functools.partial(glu_kernel, at),
        in_specs=[SMEM] + [VMEM] * 9 + [ANY, ANY],
        out_specs=[VMEM] * 3,
        scratch_shapes=[
            pltpu.VMEM((2, 4, 4, 256, 512), BF16),
            pltpu.SemaphoreType.DMA((2, 4)),
        ],
        out_shape=[
            jax.ShapeDtypeStruct((T, 256), BF16),
            jax.ShapeDtypeStruct((T, 256), BF16),
            jax.ShapeDtypeStruct((2 * HALO, 256), BF16),
        ],
        cost_estimate=pl.CostEstimate(
            flops=2 * T * 4096 * 1024, bytes_accessed=10 * 2**20, transcendentals=0
        ),
        name="glu",
    )(ix, *xp, gain.reshape(8, 1, 512), w_own, w_oth)


def conv_kernel(edge, own, oth, lim, taps, bias, low, high, ext):
    for j in range(4):
        cols = slice(j % 2 * 128, j % 2 * 128 + 128)
        ext[j, HALO:, :] = (own, oth)[j // 2][:, cols].astype(F32)
        rows = slice((1 - j // 2) * HALO, (2 - j // 2) * HALO)
        ext[j, :HALO, :] = edge[rows, cols].astype(F32)
    lane = lax.broadcasted_iota(jnp.int32, (32, 128), 1)
    row = lax.broadcasted_iota(jnp.int32, (32, 128), 0)
    means = [jnp.zeros((1, 128), F32), jnp.zeros((1, 128), F32)]
    for r in range(0, T, 32):
        reach = lim[r : r + 32, :]
        acc = [jnp.broadcast_to(bias[:, j * 128 : (j + 1) * 128], (32, 128)) for j in range(4)]
        for i in range(TAPS):
            keep = reach >= (TAPS - 1 - i)
            at = r + HALO - (TAPS - 1) + i
            for j in range(4):
                term = ext[j, at : at + 32, :] * taps[i : i + 1, j * 128 : (j + 1) * 128]
                acc[j] = acc[j] + jnp.where(keep, term, 0.0)
        mean = jnp.sum(acc[0] + acc[1] + acc[2] + acc[3], axis=1, keepdims=True) / 512.0
        mean = mean.astype(BF16).astype(F32)
        for j in range(4):
            cols = slice(j % 2 * 128, j % 2 * 128 + 128)
            (low, high)[j // 2][r : r + 32, cols] = (acc[j] - mean).astype(BF16)
        spot = jnp.where(lane == row + r % 128, mean, 0.0)
        means[r // 128] = means[r // 128] + jnp.sum(spot, axis=0, keepdims=True)
    pick = lax.broadcasted_iota(jnp.int32, (16, 128), 0)
    tail = jnp.where(pick == 0, means[0], jnp.where(pick == 1, means[1], 0.0))
    low[T:, :128] = tail.astype(BF16)
    low[T:, 128:] = jnp.zeros((16, 128), BF16)


def conv_call(edge, own, oth, lim, taps, bias):
    return pl.pallas_call(
        conv_kernel,
        out_shape=[
            jax.ShapeDtypeStruct((T + 16, 256), BF16),
            jax.ShapeDtypeStruct((T, 256), BF16),
        ],
        scratch_shapes=[pltpu.VMEM((4, HALO + T, 128), F32)],
        cost_estimate=pl.CostEstimate(flops=10**9, bytes_accessed=2**20, transcendentals=0),
        name="conv",
    )(edge, own, oth, lim, taps, bias)


def mix_kernel(at, ix, *refs):
    cp, gb, state, w_own, w_oth, outs, conv, buf, sem = (
        refs[:8], refs[8], refs[9:11], refs[11], refs[12], refs[13:15], *refs[15:]
    )
    x, c = ix[0], ix[3]
    copies = [
        fetch(w, (x - d) & 3, 128, at, buf.at[h, n], sem.at[h, n])
        for n, d in enumerate(ARRIVAL)
        for h, w in enumerate((w_own, w_oth))
    ]
    lane = lax.broadcasted_iota(jnp.int32, (T, 128), 1)
    row = lax.broadcasted_iota(jnp.int32, (T, 128), 0)
    spot = lane == (row & 127)
    total = jnp.zeros((T, 128), F32)
    for d in range(4):
        tail = cp[2 * d][T : T + 16, :128].astype(F32)
        mine = jnp.where(row < 128, tail[0:1, :], tail[1:2, :])
        mean = jnp.sum(jnp.where(spot, mine, 0.0), axis=1, keepdims=True)
        for k in range(4):
            part = cp[2 * d + k // 2][:T, k % 2 * 128 : k % 2 * 128 + 128].astype(F32) + mean
            conv[d, :, k * 128 : (k + 1) * 128] = part
            total = total + part
    mu = jnp.sum(total, axis=1, keepdims=True) / 2048.0
    square = jnp.zeros((T, 128), F32)
    for d in range(4):
        for k in range(4):
            off = conv[d, :, k * 128 : (k + 1) * 128] - mu
            square = square + off * off
    inv = lax.rsqrt(jnp.sum(square, axis=1, keepdims=True) / 2048.0 + 1e-5)
    acc = [jnp.zeros((T, 512), F32)] * 2
    for n, d in enumerate(ARRIVAL):
        par = gb.at[(x - d) & 3]
        y = (conv[d] - mu) * inv * par[0:1, :] + par[1:2, :]
        mixed = (y * jax.nn.sigmoid(y)).astype(BF16)
        for h in range(2):
            copies[2 * n + h].wait()
            acc[h] = acc[h] + dot(mixed, in_order(buf.at[h, n], c))
    for h in range(2):
        outs[h][...] = (state[h][...].astype(F32) + acc[h]).astype(BF16)


def mix_call(ix, cp, gb, state, w_own, w_oth, at):
    return pl.pallas_call(
        functools.partial(mix_kernel, at),
        in_specs=[SMEM] + [VMEM] * 11 + [ANY, ANY],
        out_specs=[VMEM] * 2,
        scratch_shapes=[
            pltpu.VMEM((4, T, 512), F32),
            pltpu.VMEM((2, 4, 4, 128, 512), BF16),
            pltpu.SemaphoreType.DMA((2, 4)),
        ],
        out_shape=[jax.ShapeDtypeStruct((T, 512), BF16)] * 2,
        cost_estimate=pl.CostEstimate(
            flops=2 * T * 2048 * 1024, bytes_accessed=6 * 2**20, transcendentals=0
        ),
        name="mix",
    )(ix, *cp, gb, *state, w_own, w_oth)


def per_device(
    hidden, doc_ids, norm_gain, w_value, w_gate, conv_taps, conv_bias, chan_gain, chan_bias, w_out
):
    x, y, z, c = (lax.axis_index(n) for n in ("x", "y", "z", "c"))
    ix = jnp.stack([x, y, z, c]).astype(jnp.int32)

    pair = jnp.concatenate([w_value, w_gate], axis=2)
    early = jnp.concatenate([pair[0], pair[1], w_out[0]], axis=0)
    late = jnp.concatenate([pair[2], w_out[1], w_out[2]], axis=0)
    early = lax.all_gather(early, ("z", "y"), axis=0)
    late = lax.all_gather(late, ("z", "y"), axis=0)
    first = to_all(hidden, ("x", "c"))

    own = lax.dynamic_slice_in_dim(hidden, c * T, T, 0)
    state = (own, swap(lax.dynamic_slice_in_dim(hidden, (1 - c) * T, T, 0)))

    small = jnp.concatenate(
        [conv_taps.reshape(LAYERS * TAPS, 256), conv_bias, chan_gain, chan_bias], axis=0
    )
    small = jnp.concatenate([small, swap(small)], axis=1)
    taps = small[: LAYERS * TAPS].reshape(LAYERS, TAPS, 512)
    bias = small[LAYERS * TAPS : LAYERS * TAPS + LAYERS]
    norm2 = to_all(small[LAYERS * TAPS + LAYERS :], "x").reshape(4, 2, LAYERS, 512)

    onward = [(i, i + 1) for i in range(15)]
    behind = lax.ppermute(doc_ids[-HALO:] + 1, ("z", "y"), onward) - 1
    docs = jnp.concatenate([behind, doc_ids])
    docs = lax.dynamic_slice_in_dim(docs, c * T, HALO + T, 0)
    here = docs[HALO:]
    reach = sum((docs[HALO - o : HALO - o + T] == here).astype(jnp.int32) for o in range(1, TAPS))
    lim = jnp.broadcast_to(reach[:, None], (T, 128))

    early, first, state, taps, bias, norm2, lim = lax.optimization_barrier(
        (early, first, state, taps, bias, norm2, lim)
    )

    blocks = [(i, i + 1) for i in range(31)]
    for l in range(LAYERS):
        if l == 0:
            own, other = first_glu_call(ix, first, norm_gain[l], early)
            oth = swap(other)
            edge = jnp.concatenate([own[-HALO:], oth[-HALO:]], axis=0)
        else:
            at = (early, early2, 1) if l == 1 else (late, late2, 0)
            own, oth, edge = glu_call(ix, ring(*state), norm_gain[l], *at)
        edge = lax.ppermute(edge, ("z", "y", "c"), blocks)
        if l == 0:
            early, edge = lax.optimization_barrier((early, edge))
            early2 = swap(early)
        if l == 1:
            late, edge = lax.optimization_barrier((late, edge))
            late2 = swap(late)
        dev = conv_call(edge, own, oth, lim, taps[l], bias[l : l + 1])
        at = (early, early2, 4) if l == 0 else (late, late2, l + 1)
        state = mix_call(ix, ring(*dev), norm2[:, :, l], state, *at)

    own, oth = state[0], swap(state[1])
    low = jnp.where(c == 0, own, oth)
    high = jnp.where(c == 0, oth, own)
    return jnp.concatenate([low, high], axis=0)


def solution(mesh):
    fine = Mesh(mesh.devices.reshape(4, 4, 4, 2), ("z", "y", "x", "c"))
    sp, tp = ("z", "y"), ("x", "c")
    placed = (
        P(sp, tp),
        P(sp),
        P(),
        P(None, sp, tp),
        P(None, sp, tp),
        P(None, None, tp),
        P(None, tp),
        P(None, tp),
        P(None, tp),
        P(None, sp, tp),
    )
    return jax.shard_map(
        per_device, mesh=fine, in_specs=placed, out_specs=P(sp, tp), check_vma=False
    )
```

```python
import functools

import jax
import jax.numpy as jnp
from jax import lax
from jax.experimental import pallas as pl
from jax.experimental.pallas import tpu as pltpu
from jax.sharding import Mesh, PartitionSpec as P


LAYERS = 3
T = 192
HALO = 32
TAPS = 31
F32 = jnp.float32
BF16 = jnp.bfloat16

SMEM = pl.BlockSpec(memory_space=pltpu.SMEM)
VMEM = pl.BlockSpec(memory_space=pltpu.VMEM)
ANY = pl.BlockSpec(memory_space=pl.ANY)


def swap(a):
    return lax.ppermute(a, "c", [(0, 1), (1, 0)])


def shift(a, by, axis="x"):
    return lax.ppermute(a, axis, [(i, (i + by) % 4) for i in range(4)])


def near(a, b, axis):
    left_a, right_b = shift(a, 1, axis), shift(b, 3, axis)
    left_b, right_a = shift(b, 1, axis), shift(a, 3, axis)
    return a, b, left_a, left_b, right_a, right_b


def far(halves, axis):
    a, b, left_a, left_b, right_a, right_b = halves
    two = shift(left_a, 1, axis), shift(right_b, 3, axis)
    return a, b, left_a, left_b, *two, right_a, right_b


def ring(a, b, axis="x"):
    return far(near(a, b, axis), axis)


def around(a, axis="x"):
    two, one, three = shift(a, 2, axis), shift(a, 1, axis), shift(a, 3, axis)
    return a, one, two, three


def to_all(a, axis):
    n = lax.axis_size(axis)
    return lax.all_to_all(jnp.broadcast_to(a[None], (n, *a.shape)), axis, 0, 0, tiled=True)


def dot(a, b):
    return jnp.dot(a, b, preferred_element_type=F32)


def in_order(w, c):
    return jnp.concatenate([w[2 * c], w[2 * c + 1], w[2 - 2 * c], w[3 - 2 * c]], axis=0)


def first_glu_kernel(ix, xp, gain, *refs):
    value, gate = refs[:8], refs[8:16]
    mine, other, own, oth, xs = refs[16:]
    x, y, z, c = ix[0], ix[1], ix[2], ix[3]
    square = jnp.zeros((2 * T, 256), F32)
    for n in range(16):
        xf = xp[n].astype(F32)
        square = square + xf * xf
        xs[n] = (xf * gain[n]).astype(BF16)
    scale = lax.rsqrt(jnp.sum(square, axis=1, keepdims=True) / 4096.0 + 1e-6)

    def rows(e, d):
        return xs[((z - e) & 3) * 4 + ((y - d) & 3)]

    acc = [jnp.zeros((2 * T, 256), F32)] * 2
    for n in range(4):
        for k, (pieces, at) in enumerate(((value, lambda m: rows(n, m)), (gate, lambda m: rows(m, n)))):
            r = jnp.concatenate([at(m) for m in range(4)], axis=1)
            w = jnp.concatenate([pieces[2 * n + m // 2][m % 2] for m in range(4)], axis=0)
            acc[k] = acc[k] + dot(r, w)
    glu = (acc[0] * scale * jax.nn.sigmoid(acc[1] * scale)).astype(BF16)
    low, high = glu[:T], glu[T:]
    mine[...] = jnp.where(c == 0, low, high)
    other[...] = jnp.where(c == 0, high, low)
    for out, core in ((own, c), (oth, 1 - c)):
        for q in range(2):
            block = xp.at[x * 4 + core * 2 + q]
            out[:, q * 256 : (q + 1) * 256] = jnp.where(c == 0, block[:T, :], block[T:, :])


def first_glu_call(ix, xp, gain, value, gate):
    return pl.pallas_call(
        first_glu_kernel,
        in_specs=[SMEM] + [VMEM] * 18,
        out_specs=[VMEM] * 4,
        scratch_shapes=[pltpu.VMEM((16, 2 * T, 256), BF16)],
        out_shape=[
            *[jax.ShapeDtypeStruct((T, 256), BF16)] * 2,
            *[jax.ShapeDtypeStruct((T, 512), BF16)] * 2,
        ],
        cost_estimate=pl.CostEstimate(
            flops=2 * T * 4096 * 1024, bytes_accessed=8 * 2**20, transcendentals=0
        ),
        compiler_params=pltpu.CompilerParams(vmem_limit_bytes=16 * 2**20),
        name="glu0",
    )(ix, xp, gain.reshape(16, 1, 256), *value, *gate)


def reach_kernel(ix, behind, docs, lim):
    start = (ix[1] == 0) & (ix[2] == 0)
    before = jnp.where(start, -1.0, behind[...].astype(F32))
    ids = jnp.concatenate([before, docs[...].astype(F32)], axis=1)
    reach = jnp.zeros((1, 768), F32)
    for o in range(1, TAPS):
        reach = reach + jnp.where(pltpu.roll(ids, o, 1) == ids, 1.0, 0.0)
    lane = lax.broadcasted_iota(jnp.int32, (T, 384), 1)
    row = lax.broadcasted_iota(jnp.int32, (T, 384), 0)
    spot = jnp.where(lane == row + ix[3] * T, reach[:, 384:], 0.0)
    lim[...] = jnp.broadcast_to(jnp.sum(spot, axis=1, keepdims=True), (T, 128))


def reach_call(ix, behind, docs):
    return pl.pallas_call(
        reach_kernel,
        in_specs=[SMEM, VMEM, VMEM],
        out_specs=VMEM,
        out_shape=jax.ShapeDtypeStruct((T, 128), F32),
        compiler_params=pltpu.CompilerParams(vmem_limit_bytes=2 * 2**20),
        name="reach",
    )(ix, behind.reshape(1, -1), docs.reshape(1, -1))


def fetch(src, row, rows, at, dst, sem):
    first = pl.multiple_of(row * 4, 4)
    copy = pltpu.make_async_copy(src.at[pl.ds(first, 4), pl.ds(at * rows, rows), :], dst, sem)
    copy.start()
    return copy


ARRIVAL = (0, 1, 3, 2)


def glu_kernel(at, ix, *refs):
    xp, gain, w_own, w_oth, own, oth, edge, buf, sem = refs[:8], *refs[8:]
    x, c = ix[0], ix[3]
    copies = [
        fetch(w, (x - d) & 3, 256, at, buf.at[h, n], sem.at[h, n])
        for n, d in enumerate(ARRIVAL)
        for h, w in enumerate((w_own, w_oth))
    ]
    square = jnp.zeros((T, 1), F32)
    acc = [jnp.zeros((T, 512), F32)] * 2
    for n, d in enumerate(ARRIVAL):
        parts = []
        for h, core in ((0, c), (1, 1 - c)):
            xf = xp[2 * d + h][...].astype(F32)
            square = square + jnp.sum(xf * xf, axis=1, keepdims=True)
            parts.append((xf * gain[((x - d) & 3) * 2 + core]).astype(BF16))
        rows = jnp.concatenate(parts, axis=1)
        for h in range(2):
            copies[2 * n + h].wait()
            acc[h] = acc[h] + dot(rows, in_order(buf.at[h, n], c))
    scale = lax.rsqrt(square / 4096.0 + 1e-6)
    for h, out in enumerate((own, oth)):
        y = acc[h] * scale
        glu = (y[:, :256] * jax.nn.sigmoid(y[:, 256:])).astype(BF16)
        out[...] = glu
        edge[h * HALO : (h + 1) * HALO, :] = glu[T - HALO :, :]


def glu_call(ix, xp, gain, w_own, w_oth, at):
    return pl.pallas_call(
        functools.partial(glu_kernel, at),
        in_specs=[SMEM] + [VMEM] * 9 + [ANY, ANY],
        out_specs=[VMEM] * 3,
        scratch_shapes=[
            pltpu.VMEM((2, 4, 4, 256, 512), BF16),
            pltpu.SemaphoreType.DMA((2, 4)),
        ],
        out_shape=[
            jax.ShapeDtypeStruct((T, 256), BF16),
            jax.ShapeDtypeStruct((T, 256), BF16),
            jax.ShapeDtypeStruct((2 * HALO, 256), BF16),
        ],
        cost_estimate=pl.CostEstimate(
            flops=2 * T * 4096 * 1024, bytes_accessed=10 * 2**20, transcendentals=0
        ),
        compiler_params=pltpu.CompilerParams(vmem_limit_bytes=16 * 2**20),
        name="glu",
    )(ix, *xp, gain.reshape(8, 1, 512), w_own, w_oth)


def conv_kernel(l, edge, own, oth, lim, taps_own, taps_oth, chan_own, chan_oth, out, ext):
    taps = (taps_own, taps_own, taps_oth, taps_oth)
    chan = (chan_own, chan_own, chan_oth, chan_oth)
    cols = (slice(0, 128), slice(128, 256)) * 2
    for j in range(4):
        ext[j, HALO:, :] = (own, oth)[j // 2][:, cols[j]].astype(F32)
        rows = slice((1 - j // 2) * HALO, (2 - j // 2) * HALO)
        ext[j, :HALO, :] = edge[rows, cols[j]].astype(F32)
    lane = lax.broadcasted_iota(jnp.int32, (32, 128), 1)
    row = lax.broadcasted_iota(jnp.int32, (32, 128), 0)
    means = [jnp.zeros((1, 128), F32), jnp.zeros((1, 128), F32)]
    for r in range(0, T, 32):
        reach = lim[r : r + 32, :]
        acc = [jnp.broadcast_to(chan[j][0, l : l + 1, cols[j]], (32, 128)) for j in range(4)]
        for i in range(TAPS):
            keep = reach >= float(TAPS - 1 - i)
            at = r + HALO - (TAPS - 1) + i
            for j in range(4):
                term = ext[j, at : at + 32, :] * taps[j][l, i : i + 1, cols[j]]
                acc[j] = acc[j] + jnp.where(keep, term, 0.0)
        mean = jnp.sum(acc[0] + acc[1] + acc[2] + acc[3], axis=1, keepdims=True) / 512.0
        mean = mean.astype(BF16).astype(F32)
        for j in range(4):
            out[r : r + 32, j * 128 : (j + 1) * 128] = (acc[j] - mean).astype(BF16)
        spot = jnp.where(lane == row + r % 128, mean, 0.0)
        means[r // 128] = means[r // 128] + jnp.sum(spot, axis=0, keepdims=True)
    pick = lax.broadcasted_iota(jnp.int32, (16, 128), 0)
    tail = jnp.where(pick == 0, means[0], jnp.where(pick == 1, means[1], 0.0))
    out[T:, :128] = tail.astype(BF16)
    out[T:, 128:] = jnp.zeros((16, 384), BF16)


def conv_call(l, *args):
    return pl.pallas_call(
        functools.partial(conv_kernel, l),
        out_shape=jax.ShapeDtypeStruct((T + 16, 512), BF16),
        scratch_shapes=[pltpu.VMEM((4, HALO + T, 128), F32)],
        cost_estimate=pl.CostEstimate(flops=10**9, bytes_accessed=2**20, transcendentals=0),
        compiler_params=pltpu.CompilerParams(vmem_limit_bytes=6 * 2**20),
        name="conv",
    )(*args)


def mix_kernel(l, at, ix, *refs):
    cp, chan, state, refs = refs[:4], refs[4:8], refs[8:10], refs[10:]
    weights, outs, (conv, buf, sem) = refs[:2], refs[2:4], refs[4:]
    x, c = ix[0], ix[3]
    copies = [
        fetch(w, (x - d) & 3, 128, at[h], buf.at[h, n], sem.at[h, n])
        for n, d in enumerate(ARRIVAL)
        for h, w in enumerate(weights)
    ]
    lane = lax.broadcasted_iota(jnp.int32, (T, 128), 1)
    row = lax.broadcasted_iota(jnp.int32, (T, 128), 0)
    spot = lane == (row & 127)
    total = jnp.zeros((T, 128), F32)
    for d in range(4):
        tail = cp[d][T : T + 16, :128].astype(F32)
        mine = jnp.where(row < 128, tail[0:1, :], tail[1:2, :])
        mean = jnp.sum(jnp.where(spot, mine, 0.0), axis=1, keepdims=True)
        for k in range(4):
            part = cp[d][:T, k * 128 : (k + 1) * 128].astype(F32) + mean
            conv[d, :, k * 128 : (k + 1) * 128] = part
            total = total + part
    mu = jnp.sum(total, axis=1, keepdims=True) / 2048.0
    square = jnp.zeros((T, 128), F32)
    for d in range(4):
        for k in range(4):
            off = conv[d, :, k * 128 : (k + 1) * 128] - mu
            square = square + off * off
    inv = lax.rsqrt(jnp.sum(square, axis=1, keepdims=True) / 2048.0 + 1e-5)
    acc = [jnp.zeros((T, 512), F32)] * 2
    for n, d in enumerate(ARRIVAL):
        par = [
            jnp.concatenate([chan[d][h, k, l : l + 1, :] for h in range(2)], axis=1)
            for k in (1, 2)
        ]
        v = (conv[d] - mu) * inv * par[0] + par[1]
        mixed = (v * jax.nn.sigmoid(v)).astype(BF16)
        for h in range(2):
            copies[2 * n + h].wait()
            acc[h] = acc[h] + dot(mixed, in_order(buf.at[h, n], c))
    for h in range(2):
        outs[h][...] = (state[h][...].astype(F32) + acc[h]).astype(BF16)


def mix_call(l, ix, cp, chan, state, weights, at):
    return pl.pallas_call(
        functools.partial(mix_kernel, l, at),
        in_specs=[SMEM] + [VMEM] * 10 + [ANY] * 2,
        out_specs=[VMEM] * 2,
        scratch_shapes=[
            pltpu.VMEM((4, T, 512), F32),
            pltpu.VMEM((2, 4, 4, 128, 512), BF16),
            pltpu.SemaphoreType.DMA((2, 4)),
        ],
        out_shape=[jax.ShapeDtypeStruct((T, 512), BF16)] * 2,
        cost_estimate=pl.CostEstimate(
            flops=2 * T * 2048 * 1024, bytes_accessed=6 * 2**20, transcendentals=0
        ),
        compiler_params=pltpu.CompilerParams(vmem_limit_bytes=12 * 2**20),
        name="mix",
    )(ix, *cp, *chan, *state, *weights)


def layers(
    hidden, doc_ids, norm_gain, w_value, w_gate, conv_taps, conv_bias, chan_gain, chan_bias, w_out
):
    x, y, z, c = (lax.axis_index(n) for n in ("x", "y", "z", "c"))
    ix = jnp.stack([x, y, z, c]).astype(jnp.int32)

    def pair(l):
        return jnp.concatenate([w_value[l], w_gate[l]], axis=1)

    def all_rows(*parts):
        return lax.all_gather(jnp.concatenate(parts, axis=0), ("z", "y"), axis=0)

    middle = all_rows(pair(1), w_out[0], w_out[1])
    blocks = jnp.moveaxis(hidden.reshape(2 * T, 2, 256), 1, 0)
    first = to_all(blocks, ("x", "c")).reshape(16, 2 * T, 256)

    value, gate = around(w_value[0], "y"), around(w_gate[0], "z")
    value, gate = jnp.stack(value), jnp.stack(gate)
    value, gate = near(value[:2], value[2:], "z"), near(gate[:2], gate[2:], "y")
    value, gate = far(value, "z"), far(gate, "y")

    onward = [(i, i + 1) for i in range(15)]
    behind = lax.ppermute(doc_ids, ("z", "y"), onward)
    lim = reach_call(ix, behind, doc_ids)
    taps = (conv_taps, swap(conv_taps))
    chan = jnp.stack([conv_bias, chan_gain, chan_bias])
    chan = (chan, swap(chan))
    parts = jnp.concatenate([pair(2), w_out[2]], axis=0)
    last = all_rows(parts)

    onward = [(i, i + 1) for i in range(31)]
    for l in range(LAYERS):
        if l == 0:
            own, oth, *state = first_glu_call(ix, first, norm_gain[l], value, gate)
            oth = swap(oth)
            edge = jnp.concatenate([own[-HALO:], oth[-HALO:]], axis=0)
        else:
            weights = (middle, middle2) if l == 1 else (last, last2)
            own, oth, edge = glu_call(ix, ring(*state), norm_gain[l], *weights, 0)
        edge = lax.ppermute(edge, ("z", "y", "c"), onward)
        dev = conv_call(l, edge, own, oth, lim, *taps, *chan)
        if l == 0:
            middle, dev, *chan = lax.optimization_barrier((middle, dev, *chan))
            devs = around(dev)
            norm = around(jnp.stack(chan))
            weights, at = (middle, swap(middle[:, 256:384])), (2, 0)
        else:
            devs = around(dev)
            at = (3, 3) if l == 1 else (2, 2)
        state = mix_call(l, ix, devs, norm, state, weights, at)
        if l == 0:
            middle, *state = lax.optimization_barrier((middle, *state))
            middle2 = swap(middle)
        if l == 1:
            last, *state = lax.optimization_barrier((last, *state))
            last2 = swap(last)

    own, oth = state[0], swap(state[1])
    low = jnp.where(c == 0, own, oth)
    high = jnp.where(c == 0, oth, own)
    return jnp.concatenate([low, high], axis=0)


def solution(mesh):
    fine = Mesh(mesh.devices.reshape(4, 4, 4, 2), ("z", "y", "x", "c"))
    sp, tp = ("z", "y"), ("x", "c")
    placed = (
        P(sp, tp),
        P(sp),
        P(),
        P(None, sp, tp),
        P(None, sp, tp),
        P(None, None, tp),
        P(None, tp),
        P(None, tp),
        P(None, tp),
        P(None, sp, tp),
    )
    return jax.shard_map(layers, mesh=fine, in_specs=placed, out_specs=P(sp, tp), check_vma=False)
```

```python
import functools

import jax
import jax.numpy as jnp
from jax import lax
from jax.experimental import pallas as pl
from jax.experimental.pallas import tpu as pltpu
from jax.sharding import Mesh, PartitionSpec as P


LAYERS = 3
T = 192
HALO = 32
TAPS = 31
F32 = jnp.float32
BF16 = jnp.bfloat16

SMEM = pl.BlockSpec(memory_space=pltpu.SMEM)
VMEM = pl.BlockSpec(memory_space=pltpu.VMEM)
HBM = pl.BlockSpec(memory_space=pltpu.HBM)


def swap(a):
    return lax.ppermute(a, "c", [(0, 1), (1, 0)])


def shift(a, by, axis="x"):
    return lax.ppermute(a, axis, [(i, (i + by) % 4) for i in range(4)])


def near(a, b, axis):
    left_a, right_b = shift(a, 1, axis), shift(b, 3, axis)
    left_b, right_a = shift(b, 1, axis), shift(a, 3, axis)
    return a, b, left_a, left_b, right_a, right_b


def far(halves, axis):
    a, b, left_a, left_b, right_a, right_b = halves
    two = shift(left_a, 1, axis), shift(right_b, 3, axis)
    return a, b, left_a, left_b, *two, right_a, right_b


def ring(a, b, axis="x"):
    return far(near(a, b, axis), axis)


def around(a, axis="x"):
    two, one, three = shift(a, 2, axis), shift(a, 1, axis), shift(a, 3, axis)
    return a, one, two, three


def to_all(a, axis):
    n = lax.axis_size(axis)
    return lax.all_to_all(jnp.broadcast_to(a[None], (n, *a.shape)), axis, 0, 0, tiled=True)


def dot(a, b):
    return jnp.dot(a, b, preferred_element_type=F32)


def in_order(w, c):
    return jnp.concatenate([w[2 * c], w[2 * c + 1], w[2 - 2 * c], w[3 - 2 * c]], axis=0)


def first_glu_kernel(ix, xp, gain, *refs):
    value, gate = refs[:8], refs[8:16]
    mine, other, own, oth, xs = refs[16:]
    x, y, z, c = ix[0], ix[1], ix[2], ix[3]
    square = jnp.zeros((2 * T, 256), F32)
    for n in range(16):
        xf = xp[n].astype(F32)
        square = square + xf * xf
        xs[n] = (xf * gain[n]).astype(BF16)
    scale = lax.rsqrt(jnp.sum(square, axis=1, keepdims=True) / 4096.0 + 1e-6)

    def rows(e, d):
        return xs[((z - e) & 3) * 4 + ((y - d) & 3)]

    acc = [jnp.zeros((2 * T, 256), F32)] * 2
    for n in range(4):
        for k, (pieces, at) in enumerate(((value, lambda m: rows(n, m)), (gate, lambda m: rows(m, n)))):
            r = jnp.concatenate([at(m) for m in range(4)], axis=1)
            w = jnp.concatenate([pieces[2 * n + m // 2][m % 2] for m in range(4)], axis=0)
            acc[k] = acc[k] + dot(r, w)
    glu = (acc[0] * scale * jax.nn.sigmoid(acc[1] * scale)).astype(BF16)
    low, high = glu[:T], glu[T:]
    mine[...] = jnp.where(c == 0, low, high)
    other[...] = jnp.where(c == 0, high, low)
    for out, core in ((own, c), (oth, 1 - c)):
        for q in range(2):
            block = xp.at[x * 4 + core * 2 + q]
            out[:, q * 256 : (q + 1) * 256] = jnp.where(c == 0, block[:T, :], block[T:, :])


def first_glu_call(ix, xp, gain, value, gate):
    return pl.pallas_call(
        first_glu_kernel,
        in_specs=[SMEM] + [VMEM] * 18,
        out_specs=[VMEM] * 4,
        scratch_shapes=[pltpu.VMEM((16, 2 * T, 256), BF16)],
        out_shape=[
            *[jax.ShapeDtypeStruct((T, 256), BF16)] * 2,
            *[jax.ShapeDtypeStruct((T, 512), BF16)] * 2,
        ],
        cost_estimate=pl.CostEstimate(
            flops=2 * T * 4096 * 1024, bytes_accessed=8 * 2**20, transcendentals=0
        ),
        compiler_params=pltpu.CompilerParams(vmem_limit_bytes=16 * 2**20),
        name="glu0",
    )(ix, xp, gain.reshape(16, 1, 256), *value, *gate)


def reach_kernel(ix, behind, docs, lim):
    start = (ix[1] == 0) & (ix[2] == 0)
    before = jnp.where(start, -1.0, behind[...].astype(F32))
    ids = jnp.concatenate([before, docs[...].astype(F32)], axis=1)
    reach = jnp.zeros((1, 768), F32)
    for o in range(1, TAPS):
        reach = reach + jnp.where(pltpu.roll(ids, o, 1) == ids, 1.0, 0.0)
    lane = lax.broadcasted_iota(jnp.int32, (T, 384), 1)
    row = lax.broadcasted_iota(jnp.int32, (T, 384), 0)
    spot = jnp.where(lane == row + ix[3] * T, reach[:, 384:], 0.0)
    lim[...] = jnp.broadcast_to(jnp.sum(spot, axis=1, keepdims=True), (T, 128))


def reach_call(ix, behind, docs):
    return pl.pallas_call(
        reach_kernel,
        in_specs=[SMEM, VMEM, VMEM],
        out_specs=VMEM,
        out_shape=jax.ShapeDtypeStruct((T, 128), F32),
        compiler_params=pltpu.CompilerParams(vmem_limit_bytes=2 * 2**20),
        name="reach",
    )(ix, behind.reshape(1, -1), docs.reshape(1, -1))


def fetch(src, row, rows, at, dst, sem):
    first = pl.multiple_of(row * 4, 4)
    copy = pltpu.make_async_copy(src.at[pl.ds(first, 4), pl.ds(at * rows, rows), :], dst, sem)
    copy.start()
    return copy


ARRIVAL = (0, 1, 3, 2)


def glu_kernel(at, ix, *refs):
    xp, gain, w_own, w_oth, own, oth, edge, buf, sem = refs[:8], *refs[8:]
    x, c = ix[0], ix[3]
    copies = [
        fetch(w, (x - d) & 3, 256, at, buf.at[h, n], sem.at[h, n])
        for n, d in enumerate(ARRIVAL)
        for h, w in enumerate((w_own, w_oth))
    ]
    square = jnp.zeros((T, 1), F32)
    acc = [jnp.zeros((T, 512), F32)] * 2
    for n, d in enumerate(ARRIVAL):
        parts = []
        for h, core in ((0, c), (1, 1 - c)):
            xf = xp[2 * d + h][...].astype(F32)
            square = square + jnp.sum(xf * xf, axis=1, keepdims=True)
            parts.append((xf * gain[((x - d) & 3) * 2 + core]).astype(BF16))
        rows = jnp.concatenate(parts, axis=1)
        for h in range(2):
            copies[2 * n + h].wait()
            acc[h] = acc[h] + dot(rows, in_order(buf.at[h, n], c))
    scale = lax.rsqrt(square / 4096.0 + 1e-6)
    for h, out in enumerate((own, oth)):
        y = acc[h] * scale
        glu = (y[:, :256] * jax.nn.sigmoid(y[:, 256:])).astype(BF16)
        out[...] = glu
        edge[h * HALO : (h + 1) * HALO, :] = glu[T - HALO :, :]


def glu_call(ix, xp, gain, w_own, w_oth, at):
    return pl.pallas_call(
        functools.partial(glu_kernel, at),
        in_specs=[SMEM] + [VMEM] * 9 + [HBM, HBM],
        out_specs=[VMEM] * 3,
        scratch_shapes=[
            pltpu.VMEM((2, 4, 4, 256, 512), BF16),
            pltpu.SemaphoreType.DMA((2, 4)),
        ],
        out_shape=[
            jax.ShapeDtypeStruct((T, 256), BF16),
            jax.ShapeDtypeStruct((T, 256), BF16),
            jax.ShapeDtypeStruct((2 * HALO, 256), BF16),
        ],
        cost_estimate=pl.CostEstimate(
            flops=2 * T * 4096 * 1024, bytes_accessed=10 * 2**20, transcendentals=0
        ),
        compiler_params=pltpu.CompilerParams(vmem_limit_bytes=16 * 2**20),
        name="glu",
    )(ix, *xp, gain.reshape(8, 1, 512), w_own, w_oth)


def thirds(v):
    high = v.astype(BF16)
    rest = v - high.astype(F32)
    middle = rest.astype(BF16)
    return high, middle, (rest - middle.astype(F32)).astype(BF16)


def conv_kernel(l, edge, own, oth, lim, chan_own, chan_oth, out, ext):
    chan = (chan_own, chan_own, chan_oth, chan_oth)
    cols = (slice(0, 128), slice(128, 256)) * 2
    for j in range(4):
        ext[j, HALO:, :] = (own, oth)[j // 2][:, cols[j]].astype(F32)
        rows = slice((1 - j // 2) * HALO, (2 - j // 2) * HALO)
        ext[j, :HALO, :] = edge[rows, cols[j]].astype(F32)
    lane = lax.broadcasted_iota(jnp.int32, (32, 128), 1)
    row = lax.broadcasted_iota(jnp.int32, (32, 128), 0)
    pick = lax.broadcasted_iota(jnp.int32, (16, 128), 0)

    def chunk(n, tail):
        r = pl.multiple_of(n * 32, 32)
        reach = lim[pl.ds(r, 32), :]
        acc = [jnp.broadcast_to(chan[j][l, TAPS : TAPS + 1, cols[j]], (32, 128)) for j in range(4)]
        for i in range(TAPS):
            keep = reach >= float(TAPS - 1 - i)
            for j in range(4):
                term = ext[j, pl.ds(r + (HALO - TAPS + 1 + i), 32), :]
                term = term * chan[j][l, i : i + 1, cols[j]]
                acc[j] = acc[j] + jnp.where(keep, term, 0.0)
        mean = jnp.sum(acc[0] + acc[1] + acc[2] + acc[3], axis=1, keepdims=True) / 512.0
        mean = mean.astype(BF16).astype(F32)
        for j in range(4):
            out[pl.ds(r, 32), j * 128 : (j + 1) * 128] = (acc[j] - mean).astype(BF16)
        spot = jnp.where(lane == row + n % 4 * 32, mean, 0.0)
        spot = jnp.sum(spot, axis=0, keepdims=True)
        return tail + jnp.where(pick == n // 4, spot, 0.0)

    tail = lax.fori_loop(0, T // 32, chunk, jnp.zeros((16, 128), F32)).astype(BF16)
    for j in range(4):
        block = tail if j == 0 else jnp.zeros((16, 128), BF16)
        at = 2
        for k in (1, 2):
            for part in thirds(chan[j][l, TAPS + k : TAPS + k + 1, cols[j]]):
                block = jnp.where(pick == at, jnp.broadcast_to(part.astype(F32), (16, 128)), block.astype(F32)).astype(BF16)
                at += 1
        out[T:, j * 128 : (j + 1) * 128] = block


def conv_call(l, *args):
    return pl.pallas_call(
        functools.partial(conv_kernel, l),
        out_shape=jax.ShapeDtypeStruct((T + 16, 512), BF16),
        scratch_shapes=[pltpu.VMEM((4, HALO + T, 128), F32)],
        cost_estimate=pl.CostEstimate(flops=10**9, bytes_accessed=2**20, transcendentals=0),
        compiler_params=pltpu.CompilerParams(vmem_limit_bytes=6 * 2**20),
        name="conv",
    )(*args)


def mix_kernel(at, ix, *refs):
    cp, state, refs = refs[:4], refs[4:6], refs[6:]
    weights, outs, (mixed, buf, sem) = refs[:2], refs[2:4], refs[4:]
    x, c = ix[0], ix[3]
    copies = [
        fetch(w, (x - d) & 3, 128, at[h], buf.at[h, n], sem.at[h, n])
        for n, d in enumerate(ARRIVAL)
        for h, w in enumerate(weights)
    ]
    lane = lax.broadcasted_iota(jnp.int32, (64, 128), 1)
    row = lax.broadcasted_iota(jnp.int32, (64, 128), 0)

    def chunk(n, carry):
        r = pl.multiple_of(n * 64, 64)
        spot = lane == row + n % 2 * 64
        means, total = [], jnp.zeros((64, 128), F32)

        def part(d, k):
            return cp[d][pl.ds(r, 64), k * 128 : (k + 1) * 128].astype(F32) + means[d]

        for d in range(4):
            tail = cp[d][T : T + 16, :128].astype(F32)
            mine = jnp.where(n < 2, tail[0:1, :], tail[1:2, :])
            means.append(jnp.sum(jnp.where(spot, mine, 0.0), axis=1, keepdims=True))
            for k in range(4):
                total = total + part(d, k)
        mu = jnp.sum(total, axis=1, keepdims=True) / 2048.0
        square = jnp.zeros((64, 128), F32)
        for d in range(4):
            for k in range(4):
                off = part(d, k) - mu
                square = square + off * off
        inv = lax.rsqrt(jnp.sum(square, axis=1, keepdims=True) / 2048.0 + 1e-5)
        for d in range(4):
            for k in range(4):
                at = slice(k * 128, (k + 1) * 128)
                tail = cp[d][T:, at].astype(F32)
                gain, bias = [jnp.sum(tail[m : m + 3, :], axis=0, keepdims=True) for m in (2, 5)]
                v = (part(d, k) - mu) * inv * gain + bias
                mixed[d, pl.ds(r, 64), at] = (v * jax.nn.sigmoid(v)).astype(BF16)
        return carry

    lax.fori_loop(0, T // 64, chunk, 0)
    acc = [jnp.zeros((T, 512), F32)] * 2
    for n, d in enumerate(ARRIVAL):
        for h in range(2):
            copies[2 * n + h].wait()
            acc[h] = acc[h] + dot(mixed[d], in_order(buf.at[h, n], c))
    for h in range(2):
        outs[h][...] = (state[h][...].astype(F32) + acc[h]).astype(BF16)


def mix_call(ix, cp, state, weights, at):
    return pl.pallas_call(
        functools.partial(mix_kernel, at),
        in_specs=[SMEM] + [VMEM] * 6 + [HBM] * 2,
        out_specs=[VMEM] * 2,
        scratch_shapes=[
            pltpu.VMEM((4, T, 512), BF16),
            pltpu.VMEM((2, 4, 4, 128, 512), BF16),
            pltpu.SemaphoreType.DMA((2, 4)),
        ],
        out_shape=[jax.ShapeDtypeStruct((T, 512), BF16)] * 2,
        cost_estimate=pl.CostEstimate(
            flops=2 * T * 2048 * 1024, bytes_accessed=6 * 2**20, transcendentals=0
        ),
        compiler_params=pltpu.CompilerParams(vmem_limit_bytes=12 * 2**20),
        name="mix",
    )(ix, *cp, *state, *weights)


def layers(
    hidden, doc_ids, norm_gain, w_value, w_gate, conv_taps, conv_bias, chan_gain, chan_bias, w_out
):
    x, y, z, c = (lax.axis_index(n) for n in ("x", "y", "z", "c"))
    ix = jnp.stack([x, y, z, c]).astype(jnp.int32)

    def pair(l):
        return jnp.concatenate([w_value[l], w_gate[l]], axis=1)

    def all_rows(*parts):
        return lax.all_gather(jnp.concatenate(parts, axis=0), ("z", "y"), axis=0)

    middle = all_rows(pair(1), w_out[0], w_out[1])
    blocks = jnp.moveaxis(hidden.reshape(2 * T, 2, 256), 1, 0)
    first = to_all(blocks, ("x", "c")).reshape(16, 2 * T, 256)

    value, gate = around(w_value[0], "y"), around(w_gate[0], "z")
    value, gate = jnp.stack(value), jnp.stack(gate)
    value, gate = near(value[:2], value[2:], "z"), near(gate[:2], gate[2:], "y")
    value, gate = far(value, "z"), far(gate, "y")

    onward = [(i, i + 1) for i in range(15)]
    behind = lax.ppermute(doc_ids, ("z", "y"), onward)
    lim = reach_call(ix, behind, doc_ids)
    rows = [v[:, None] for v in (conv_bias, chan_gain, chan_bias)]
    chan = jnp.concatenate([conv_taps, *rows], axis=1)
    chan = (chan, swap(chan))
    parts = jnp.concatenate([pair(2), w_out[2]], axis=0)
    last = all_rows(parts)

    onward = [(i, i + 1) for i in range(31)]
    for l in range(LAYERS):
        if l == 0:
            own, oth, *state = first_glu_call(ix, first, norm_gain[l], value, gate)
            oth = swap(oth)
            edge = jnp.concatenate([own[-HALO:], oth[-HALO:]], axis=0)
        else:
            weights = weights if l == 1 else last
            own, oth, edge = glu_call(ix, ring(*state), norm_gain[l], *weights, 0)
        edge = lax.ppermute(edge, ("z", "y", "c"), onward)
        dev = conv_call(l, edge, own, oth, lim, *chan)
        if l == 0:
            part = middle[:, 256:384]
            part = swap(part)
            middle, part = lax.optimization_barrier((middle, part))
            weights = (middle, swap(middle))
        devs = around(dev)
        with_out = ((middle, part), (2, 0)) if l == 0 else (weights, (4 - l, 4 - l))
        state = mix_call(ix, devs, state, *with_out)
        if l == 1:
            last, *state = lax.optimization_barrier((last, *state))
            last = (last, swap(last))

    own, oth = state[0], swap(state[1])
    low = jnp.where(c == 0, own, oth)
    high = jnp.where(c == 0, oth, own)
    return jnp.concatenate([low, high], axis=0)


def solution(mesh):
    fine = Mesh(mesh.devices.reshape(4, 4, 4, 2), ("z", "y", "x", "c"))
    sp, tp = ("z", "y"), ("x", "c")
    placed = (
        P(sp, tp),
        P(sp),
        P(),
        P(None, sp, tp),
        P(None, sp, tp),
        P(None, None, tp),
        P(None, tp),
        P(None, tp),
        P(None, tp),
        P(None, sp, tp),
    )
    return jax.shard_map(layers, mesh=fine, in_specs=placed, out_specs=P(sp, tp), check_vma=False)
```

```python
import functools

import jax
import jax.numpy as jnp
from jax import lax
from jax.experimental import pallas as pl
from jax.experimental.pallas import tpu as pltpu
from jax.sharding import Mesh, PartitionSpec as P


LAYERS = 3
T = 192
HALO = 32
TAPS = 31
F32 = jnp.float32
BF16 = jnp.bfloat16

SMEM = pl.BlockSpec(memory_space=pltpu.SMEM)
VMEM = pl.BlockSpec(memory_space=pltpu.VMEM)
HBM = pl.BlockSpec(memory_space=pltpu.HBM)


def in_hbm(a):
    return pltpu.with_memory_space_constraint(a, pltpu.HBM)


def swap(a):
    return lax.ppermute(a, "c", [(0, 1), (1, 0)])


def shift(a, by, axis="x"):
    return lax.ppermute(a, axis, [(i, (i + by) % 4) for i in range(4)])


def near(a, b, axis):
    left_a, right_b = shift(a, 1, axis), shift(b, 3, axis)
    left_b, right_a = shift(b, 1, axis), shift(a, 3, axis)
    return a, b, left_a, left_b, right_a, right_b


def far(halves, axis):
    a, b, left_a, left_b, right_a, right_b = halves
    two = shift(left_a, 1, axis), shift(right_b, 3, axis)
    return a, b, left_a, left_b, *two, right_a, right_b


def around(a, axis="x"):
    two, one, three = shift(a, 2, axis), shift(a, 1, axis), shift(a, 3, axis)
    return a, one, two, three


def to_all(a, axis):
    n = lax.axis_size(axis)
    return lax.all_to_all(jnp.broadcast_to(a[None], (n, *a.shape)), axis, 0, 0, tiled=True)


def dot(a, b):
    return jnp.dot(a, b, preferred_element_type=F32)


def in_order(w, c):
    return jnp.concatenate([w[2 * c], w[2 * c + 1], w[2 - 2 * c], w[3 - 2 * c]], axis=0)


def first_glu_kernel(ix, xp, gain, *refs):
    value, gate = refs[:8], refs[8:16]
    mine, other, own, oth, xs = refs[16:]
    x, y, z, c = ix[0], ix[1], ix[2], ix[3]
    square = jnp.zeros((2 * T, 256), F32)
    for n in range(16):
        xf = xp[n].astype(F32)
        square = square + xf * xf
        xs[n] = (xf * gain[n]).astype(BF16)
    scale = lax.rsqrt(jnp.sum(square, axis=1, keepdims=True) / 4096.0 + 1e-6)

    def rows(e, d):
        return xs[((z - e) & 3) * 4 + ((y - d) & 3)]

    acc = [jnp.zeros((2 * T, 256), F32)] * 2
    for n in range(4):
        for k, (pieces, at) in enumerate(((value, lambda m: rows(n, m)), (gate, lambda m: rows(m, n)))):
            r = jnp.concatenate([at(m) for m in range(4)], axis=1)
            w = jnp.concatenate([pieces[2 * n + m // 2][m % 2] for m in range(4)], axis=0)
            acc[k] = acc[k] + dot(r, w)
    glu = (acc[0] * scale * jax.nn.sigmoid(acc[1] * scale)).astype(BF16)
    low, high = glu[:T], glu[T:]
    mine[...] = jnp.where(c == 0, low, high)
    other[...] = jnp.where(c == 0, high, low)
    for out, core in ((own, c), (oth, 1 - c)):
        for q in range(2):
            block = xp.at[x * 4 + core * 2 + q]
            out[:, q * 256 : (q + 1) * 256] = jnp.where(c == 0, block[:T, :], block[T:, :])


def first_glu_call(ix, xp, gain, value, gate):
    return pl.pallas_call(
        first_glu_kernel,
        in_specs=[SMEM] + [VMEM] * 18,
        out_specs=[VMEM] * 4,
        scratch_shapes=[pltpu.VMEM((16, 2 * T, 256), BF16)],
        out_shape=[
            *[jax.ShapeDtypeStruct((T, 256), BF16)] * 2,
            *[jax.ShapeDtypeStruct((T, 512), BF16)] * 2,
        ],
        cost_estimate=pl.CostEstimate(
            flops=2 * T * 4096 * 1024, bytes_accessed=8 * 2**20, transcendentals=0
        ),
        compiler_params=pltpu.CompilerParams(vmem_limit_bytes=16 * 2**20),
        name="glu0",
    )(ix, xp, gain.reshape(16, 1, 256), *value, *gate)


def reach_kernel(ix, behind, docs, lim):
    start = (ix[1] == 0) & (ix[2] == 0)
    before = jnp.where(start, -1.0, behind[...].astype(F32))
    ids = jnp.concatenate([before, docs[...].astype(F32)], axis=1)
    reach = jnp.zeros((1, 768), F32)
    for o in range(1, TAPS):
        reach = reach + jnp.where(pltpu.roll(ids, o, 1) == ids, 1.0, 0.0)
    lane = lax.broadcasted_iota(jnp.int32, (T, 384), 1)
    row = lax.broadcasted_iota(jnp.int32, (T, 384), 0)
    spot = jnp.where(lane == row + ix[3] * T, reach[:, 384:], 0.0)
    lim[...] = jnp.broadcast_to(jnp.sum(spot, axis=1, keepdims=True), (T, 128))


def reach_call(ix, behind, docs):
    return pl.pallas_call(
        reach_kernel,
        in_specs=[SMEM, VMEM, VMEM],
        out_specs=VMEM,
        out_shape=jax.ShapeDtypeStruct((T, 128), F32),
        compiler_params=pltpu.CompilerParams(vmem_limit_bytes=2 * 2**20),
        name="reach",
    )(ix, behind.reshape(1, -1), docs.reshape(1, -1))


def fetch(src, row, rows, at, dst, sem):
    first = pl.multiple_of(row * 4, 4)
    copy = pltpu.make_async_copy(src.at[pl.ds(first, 4), pl.ds(at * rows, rows), :], dst, sem)
    copy.start()
    return copy


ARRIVAL = (0, 1, 3, 2)


def glu_kernel(at, ix, *refs):
    xp, gain, w_own, w_oth, own, oth, edge, buf, sem = refs[:8], *refs[8:]
    x, c = ix[0], ix[3]
    copies = [
        fetch(w, (x - d) & 3, 256, at, buf.at[h, n], sem.at[h, n])
        for n, d in enumerate(ARRIVAL)
        for h, w in enumerate((w_own, w_oth))
    ]
    square = jnp.zeros((T, 1), F32)
    acc = [jnp.zeros((T, 512), F32)] * 2
    for n, d in enumerate(ARRIVAL):
        parts = []
        for h, core in ((0, c), (1, 1 - c)):
            xf = xp[2 * d + h][...].astype(F32)
            square = square + jnp.sum(xf * xf, axis=1, keepdims=True)
            parts.append((xf * gain[((x - d) & 3) * 2 + core]).astype(BF16))
        rows = jnp.concatenate(parts, axis=1)
        for h in range(2):
            copies[2 * n + h].wait()
            acc[h] = acc[h] + dot(rows, in_order(buf.at[h, n], c))
    scale = lax.rsqrt(square / 4096.0 + 1e-6)
    for h, out in enumerate((own, oth)):
        y = acc[h] * scale
        glu = (y[:, :256] * jax.nn.sigmoid(y[:, 256:])).astype(BF16)
        out[...] = glu
        edge[h * HALO : (h + 1) * HALO, :] = glu[T - HALO :, :]


def glu_call(ix, xp, gain, w_own, w_oth, at):
    return pl.pallas_call(
        functools.partial(glu_kernel, at),
        in_specs=[SMEM] + [VMEM] * 9 + [HBM, HBM],
        out_specs=[VMEM] * 3,
        scratch_shapes=[
            pltpu.VMEM((2, 4, 4, 256, 512), BF16),
            pltpu.SemaphoreType.DMA((2, 4)),
        ],
        out_shape=[
            jax.ShapeDtypeStruct((T, 256), BF16),
            jax.ShapeDtypeStruct((T, 256), BF16),
            jax.ShapeDtypeStruct((2 * HALO, 256), BF16),
        ],
        cost_estimate=pl.CostEstimate(
            flops=2 * T * 4096 * 1024, bytes_accessed=10 * 2**20, transcendentals=0
        ),
        compiler_params=pltpu.CompilerParams(vmem_limit_bytes=16 * 2**20),
        name="glu",
    )(ix, *xp, gain.reshape(8, 1, 512), in_hbm(w_own), w_oth)


def thirds(v):
    high = v.astype(BF16)
    rest = v - high.astype(F32)
    middle = rest.astype(BF16)
    return high, middle, (rest - middle.astype(F32)).astype(BF16)


def conv_kernel(l, edge, own, oth, lim, chan_own, chan_oth, out, ext):
    chan = (chan_own, chan_own, chan_oth, chan_oth)
    cols = (slice(0, 128), slice(128, 256)) * 2
    for j in range(4):
        ext[j, HALO:, :] = (own, oth)[j // 2][:, cols[j]].astype(F32)
        rows = slice((1 - j // 2) * HALO, (2 - j // 2) * HALO)
        ext[j, :HALO, :] = edge[rows, cols[j]].astype(F32)
    lane = lax.broadcasted_iota(jnp.int32, (32, 128), 1)
    row = lax.broadcasted_iota(jnp.int32, (32, 128), 0)
    pick = lax.broadcasted_iota(jnp.int32, (16, 128), 0)

    def chunk(n, tail):
        r = pl.multiple_of(n * 32, 32)
        reach = lim[pl.ds(r, 32), :]
        acc = [jnp.broadcast_to(chan[j][l, TAPS : TAPS + 1, cols[j]], (32, 128)) for j in range(4)]
        for i in range(TAPS):
            keep = reach >= float(TAPS - 1 - i)
            for j in range(4):
                term = ext[j, pl.ds(r + (HALO - TAPS + 1 + i), 32), :]
                term = term * chan[j][l, i : i + 1, cols[j]]
                acc[j] = acc[j] + jnp.where(keep, term, 0.0)
        mean = jnp.sum(acc[0] + acc[1] + acc[2] + acc[3], axis=1, keepdims=True) / 512.0
        mean = mean.astype(BF16).astype(F32)
        for j in range(4):
            out[pl.ds(r, 32), j * 128 : (j + 1) * 128] = (acc[j] - mean).astype(BF16)
        spot = jnp.where(lane == row + n % 4 * 32, mean, 0.0)
        spot = jnp.sum(spot, axis=0, keepdims=True)
        return tail + jnp.where(pick == n // 4, spot, 0.0)

    tail = lax.fori_loop(0, T // 32, chunk, jnp.zeros((16, 128), F32)).astype(BF16)
    for j in range(4):
        block = tail if j == 0 else jnp.zeros((16, 128), BF16)
        at = 2
        for k in (1, 2):
            for part in thirds(chan[j][l, TAPS + k : TAPS + k + 1, cols[j]]):
                block = jnp.where(pick == at, jnp.broadcast_to(part.astype(F32), (16, 128)), block.astype(F32)).astype(BF16)
                at += 1
        out[T:, j * 128 : (j + 1) * 128] = block


def conv_call(l, *args):
    return pl.pallas_call(
        functools.partial(conv_kernel, l),
        out_shape=jax.ShapeDtypeStruct((T + 16, 512), BF16),
        scratch_shapes=[pltpu.VMEM((4, HALO + T, 128), F32)],
        cost_estimate=pl.CostEstimate(flops=10**9, bytes_accessed=2**20, transcendentals=0),
        compiler_params=pltpu.CompilerParams(vmem_limit_bytes=6 * 2**20),
        name="conv",
    )(*args)


def mix_kernel(at, ix, *refs):
    cp, state, refs = refs[:4], refs[4:6], refs[6:]
    weights, outs, (mixed, buf, old, sem, sem2) = refs[:2], refs[2:4], refs[4:]
    x, c = ix[0], ix[3]
    copies = [
        fetch(w, (x - d) & 3, 128, at[h], buf.at[h, n], sem.at[h, n])
        for n, d in enumerate(ARRIVAL)
        for h, w in enumerate(weights)
    ]
    olds = [pltpu.make_async_copy(state[h], old.at[h], sem2.at[h]) for h in range(2)]
    for copy in olds:
        copy.start()
    lane = lax.broadcasted_iota(jnp.int32, (64, 128), 1)
    row = lax.broadcasted_iota(jnp.int32, (64, 128), 0)

    def chunk(n, carry):
        r = pl.multiple_of(n * 64, 64)
        spot = lane == row + n % 2 * 64
        means, total = [], jnp.zeros((64, 128), F32)

        def part(d, k):
            return cp[d][pl.ds(r, 64), k * 128 : (k + 1) * 128].astype(F32) + means[d]

        for d in range(4):
            tail = cp[d][T : T + 16, :128].astype(F32)
            mine = jnp.where(n < 2, tail[0:1, :], tail[1:2, :])
            means.append(jnp.sum(jnp.where(spot, mine, 0.0), axis=1, keepdims=True))
            for k in range(4):
                total = total + part(d, k)
        mu = jnp.sum(total, axis=1, keepdims=True) / 2048.0
        square = jnp.zeros((64, 128), F32)
        for d in range(4):
            for k in range(4):
                off = part(d, k) - mu
                square = square + off * off
        inv = lax.rsqrt(jnp.sum(square, axis=1, keepdims=True) / 2048.0 + 1e-5)
        for d in range(4):
            for k in range(4):
                at = slice(k * 128, (k + 1) * 128)
                tail = cp[d][T:, at].astype(F32)
                gain, bias = [jnp.sum(tail[m : m + 3, :], axis=0, keepdims=True) for m in (2, 5)]
                v = (part(d, k) - mu) * inv * gain + bias
                mixed[d, pl.ds(r, 64), at] = (v * jax.nn.sigmoid(v)).astype(BF16)
        return carry

    lax.fori_loop(0, T // 64, chunk, 0)
    acc = [jnp.zeros((T, 512), F32)] * 2
    for n, d in enumerate(ARRIVAL):
        for h in range(2):
            copies[2 * n + h].wait()
            acc[h] = acc[h] + dot(mixed[d], in_order(buf.at[h, n], c))
    for h in range(2):
        olds[h].wait()
        outs[h][...] = (old[h].astype(F32) + acc[h]).astype(BF16)


def mix_call(ix, cp, state, weights, at):
    return pl.pallas_call(
        functools.partial(mix_kernel, at),
        in_specs=[SMEM] + [VMEM] * 4 + [HBM] * 4,
        out_specs=[VMEM] * 2,
        scratch_shapes=[
            pltpu.VMEM((4, T, 512), BF16),
            pltpu.VMEM((2, 4, 4, 128, 512), BF16),
            pltpu.VMEM((2, T, 512), BF16),
            pltpu.SemaphoreType.DMA((2, 4)),
            pltpu.SemaphoreType.DMA((2,)),
        ],
        out_shape=[jax.ShapeDtypeStruct((T, 512), BF16)] * 2,
        cost_estimate=pl.CostEstimate(
            flops=2 * T * 2048 * 1024, bytes_accessed=6 * 2**20, transcendentals=0
        ),
        compiler_params=pltpu.CompilerParams(vmem_limit_bytes=12 * 2**20),
        name="mix",
    )(ix, *cp, *state, in_hbm(weights[0]), weights[1])


def layers(
    hidden, doc_ids, norm_gain, w_value, w_gate, conv_taps, conv_bias, chan_gain, chan_bias, w_out
):
    x, y, z, c = (lax.axis_index(n) for n in ("x", "y", "z", "c"))
    ix = jnp.stack([x, y, z, c]).astype(jnp.int32)

    def pair(l):
        return jnp.concatenate([w_value[l], w_gate[l]], axis=1)

    def all_rows(part):
        return lax.all_gather(part, ("z", "y"), axis=0)

    packed = jnp.concatenate([pair(1), w_out[0], w_out[1]], axis=0)
    packed, hidden = lax.optimization_barrier((packed, hidden))
    middle = all_rows(packed)
    blocks = jnp.moveaxis(hidden.reshape(2 * T, 2, 256), 1, 0)
    first = to_all(blocks, ("x", "c")).reshape(16, 2 * T, 256)

    value, gate = around(w_value[0], "y"), around(w_gate[0], "z")
    value, gate = jnp.stack(value), jnp.stack(gate)
    value, gate = near(value[:2], value[2:], "z"), near(gate[:2], gate[2:], "y")
    value, gate = far(value, "z"), far(gate, "y")

    onward = [(i, i + 1) for i in range(15)]
    behind = lax.ppermute(doc_ids, ("z", "y"), onward)
    lim = reach_call(ix, behind, doc_ids)
    rows = [v[:, None] for v in (conv_bias, chan_gain, chan_bias)]
    chan = jnp.concatenate([conv_taps, *rows], axis=1)
    chan = (chan, swap(chan))
    parts = jnp.concatenate([pair(2), w_out[2]], axis=0)
    last = all_rows(parts)

    onward = [(i, i + 1) for i in range(31)]
    for l in range(LAYERS):
        if l == 0:
            own, oth, *state = first_glu_call(ix, first, norm_gain[l], value, gate)
            oth = swap(oth)
            edge = jnp.concatenate([own[-HALO:], oth[-HALO:]], axis=0)
        else:
            weights = weights if l == 1 else last
            halves = near(*state, "x")
            blocks = far(halves, "x")
            own, oth, edge = glu_call(ix, blocks, norm_gain[l], *weights, 0)
        edge = lax.ppermute(edge, ("z", "y", "c"), onward)
        dev = conv_call(l, edge, own, oth, lim, *chan)
        if l == 0:
            part = middle[:, 256:384]
            part = swap(part)
            middle, part = lax.optimization_barrier((middle, part))
            weights = (middle, swap(middle))
            state = [in_hbm(v) for v in state]
        devs = around(dev)
        with_out = ((middle, part), (2, 0)) if l == 0 else (weights, (4 - l, 4 - l))
        state = mix_call(ix, devs, state, *with_out)
        if l == 1:
            last = (last, swap(last))

    own, oth = state[0], swap(state[1])
    low = jnp.where(c == 0, own, oth)
    high = jnp.where(c == 0, oth, own)
    return jnp.concatenate([low, high], axis=0)


def solution(mesh):
    fine = Mesh(mesh.devices.reshape(4, 4, 4, 2), ("z", "y", "x", "c"))
    sp, tp = ("z", "y"), ("x", "c")
    placed = (
        P(sp, tp),
        P(sp),
        P(),
        P(None, sp, tp),
        P(None, sp, tp),
        P(None, None, tp),
        P(None, tp),
        P(None, tp),
        P(None, tp),
        P(None, sp, tp),
    )
    return jax.shard_map(layers, mesh=fine, in_specs=placed, out_specs=P(sp, tp), check_vma=False)
```
